32 devices in a mesh: sp: 8 (over z, x), tp: 4 (over y, core).
Axes of the slice: x: 2, y: 2, z: 4, core: 2. Of those that a mesh axis runs over, the one named last changes fastest.
Arguments:
- broad_probe_tensor: bfloat16 [4096, 1024], P('sp', 'tp'), may hold values from -6 to 6
- broad_lookup_tensor: bfloat16 [4096, 1024], P('sp', 'tp'), may hold values from -6 to 6
- broad_payload_tensor: bfloat16 [4096, 1024], P('sp', 'tp'), may hold values from -6 to 6
- broad_emission_valve: bfloat16 [4096, 1024], P('sp', 'tp'), may hold values from -6 to 6
- slim_probe_tensor: bfloat16 [4096, 1024], P('sp', 'tp'), may hold values from -6 to 6
- slim_lookup_tensor: bfloat16 [4096, 1024], P('sp', 'tp'), may hold values from -6 to 6
- slim_payload_tensor: bfloat16 [4096, 1024], P('sp', 'tp'), may hold values from -6 to 6
- slim_emission_valve: bfloat16 [4096, 1024], P('sp', 'tp'), may hold values from -6 to 6
- broad_forgetting_speed: float32 [8], P('tp'), may hold values from -0.08 to 0
- slim_forgetting_speed: float32 [16], P('tp'), may hold values from -0.08 to 0
- broad_channel_scaling: float32 [1024], P('tp'), may hold values from 0.1 to 1.9
- slim_channel_scaling: float32 [1024], P('tp'), may hold values from 0.1 to 1.9
- surge_forgetting: float32 [4096], P('sp'), may hold values from -2.1 to 0
- broad_emission_proj: bfloat16 [1024, 2048], replicated, may hold values from -0.125 to 0.125
- slim_emission_proj: bfloat16 [1024, 2048], replicated, may hold values from -0.125 to 0.125
- skip_stream: bfloat16 [4096, 2048], P(('sp', 'tp')), may hold values from -6 to 6
- premix_scaling_coeffs: float32 [2048], replicated, may hold values from 0.1 to 1.9
- routed_specialist_ids: int32 [4096, 2], P('sp'), may hold values from 0 to 7, as said below
- routed_specialist_shares: float32 [4096, 2], P('sp'), may hold values from 0.2 to 1
- specialist_valve_proj: bfloat16 [8, 2048, 2048], P('sp', None, 'tp'), may hold values from -0.125 to 0.125
- specialist_expand_proj: bfloat16 [8, 2048, 2048], P('sp', None, 'tp'), may hold values from -0.125 to 0.125
- specialist_contract_proj: bfloat16 [8, 2048, 2048], P('sp', 'tp'), may hold values from -0.125 to 0.125
Outputs:
- result: bfloat16 [4096, 2048], P(('sp', 'tp'))
The draws below stay inside these ranges and needn't reach their ends.
Inputs may be any that keep to these rules, and one draw needn't show every extreme that they name: `routed_specialist_ids`: each row names two different experts of one group, that is of the same run of 2 consecutive experts. The rows of one device (each aligned block of 128 rows) name each expert at most 64 times, and some expert is named exactly 64 times by the rows of every device.
All inputs are finite; a program needn't handle non-finite values.
Results may differ from the reference program's by a relative error of at most 0.018.
Values may be sent and summed in bfloat16 or wider, within the bound.
A program may use at most 128 MiB of HBM per device.

```python
import jax
import jax.numpy as jnp
from jax import lax

D = 2048
HA = 8
BROAD_CHANNEL_DIM = 128
HB = 16
THIN_CHANNEL_DIM = 64
FFE = 2048
GROUPS = 4
EXPERTS = 8
EXP_GROUP = 2
ROWS = 128
CAP = 64
TOKENS = 4096
BLOCK = 512
N_SP = 8
N_TP = 4


def rate_law(key, heads):
    pick_key, fast_key, slow_key = jax.random.split(key, 3)
    share = 5
    fast = jax.random.randint(pick_key, (heads,), 0, 10) < share
    span = jax.random.uniform(fast_key, (heads,), jnp.float32, 30.0, 100.0)
    slow = jnp.exp(jax.random.uniform(slow_key, (heads,), jnp.float32, jnp.log(0.02), jnp.log(0.2))) / TOKENS
    return jnp.where(fast, -jnp.log(10.0) / span, -slow).astype(jnp.float32)


def draw_broad_forgetting_speed(key, part):
    return rate_law(jax.random.fold_in(key, 11), HA)


def draw_slim_forgetting_speed(key, part):
    return rate_law(jax.random.fold_in(key, 12), HB)


def draw_surge_forgetting(key, part):
    where_key, size_key = jax.random.split(jax.random.fold_in(key, 21))
    spots = jax.random.randint(where_key, (3,), 0, TOKENS)
    kept = jax.random.uniform(size_key, (3,), jnp.float32, 0.5, 0.8)
    places = jnp.arange(TOKENS, dtype=jnp.int32)
    marks = jnp.where(places[None, :] == spots[:, None], jnp.log(kept)[:, None], 0.0)
    return jnp.sum(marks, 0).astype(jnp.float32)


def draw_routed_specialist_ids(key, part):
    base = jax.random.fold_in(key, 31)
    busy = jax.random.randint(jax.random.fold_in(base, 0), (), 0, GROUPS)
    blocks = TOKENS // ROWS
    units = CAP // 2

    def one(index):
        block_key = jax.random.fold_in(base, index + 1)
        cut_key, perm_key, offset_key, stride_key = jax.random.split(block_key, 4)
        cuts = jnp.sort(jax.random.randint(cut_key, (GROUPS - 2,), 0, units + 1))
        edges = jnp.concatenate([jnp.zeros((1,), jnp.int32), cuts, jnp.full((1,), units, jnp.int32)])
        counts = jnp.concatenate([jnp.full((1,), ROWS // 2, jnp.int32), (edges[1:] - edges[:-1]) * EXP_GROUP])
        ends = jnp.cumsum(counts)
        starts = ends - counts
        slot = jax.random.permutation(perm_key, ROWS)
        order = jnp.sum((slot[:, None] >= ends[None, :]).astype(jnp.int32), 1)
        inside = slot - starts[order]
        group = (busy + order) % GROUPS
        segment_begin = jax.random.randint(offset_key, (GROUPS,), 0, EXP_GROUP)
        stride = jax.random.randint(stride_key, (GROUPS,), 1, EXP_GROUP)
        first = group * EXP_GROUP + (segment_begin[group] + inside) % EXP_GROUP
        second = group * EXP_GROUP + (segment_begin[group] + inside + stride[group]) % EXP_GROUP
        return jnp.stack([first, second], 1)
    return jax.vmap(one)(jnp.arange(blocks, dtype=jnp.int32)).reshape(TOKENS, 2).astype(jnp.int32)


def steps_of(rng, dims, shards, smallest, largest):
    loudness = 1.0
    for position, parts in shards:
        heights = jax.random.uniform(jax.random.fold_in(jax.random.fold_in(rng, 6), position), (parts,), jnp.float32, smallest / len(shards), largest / len(shards))
        loudness = loudness * jnp.repeat(jnp.exp(heights), dims[position] // parts).reshape((-1,) + (1,) * (len(dims) - 1 - position))
    return loudness


def noise(stream_key, dims, scale, limit, cuts=(), kind=jnp.bfloat16):
    loudness = steps_of(stream_key, dims, cuts, -0.22, 0.18) if cuts else 1.0
    entries = jax.random.normal(stream_key, dims, jnp.float32) * scale * loudness
    return jnp.minimum(jnp.maximum(entries, -limit), limit).astype(kind)


def setup_inputs(seed: int = 0) -> dict:
    keys = jax.random.split(jax.random.key(seed), 23)
    return {
        "broad_probe_tensor": noise(keys[0], (TOKENS, HA * BROAD_CHANNEL_DIM), 1.0, 6.0, ((0, 8), (1, 4))),
        "broad_lookup_tensor": noise(keys[1], (TOKENS, HA * BROAD_CHANNEL_DIM), 1.0, 6.0, ((0, 8), (1, 4))),
        "broad_payload_tensor": noise(keys[2], (TOKENS, HA * BROAD_CHANNEL_DIM), 1.0, 6.0, ((0, 8), (1, 4))),
        "broad_emission_valve": noise(keys[3], (TOKENS, HA * BROAD_CHANNEL_DIM), 1.0, 6.0, ((0, 8), (1, 4))),
        "slim_probe_tensor": noise(keys[4], (TOKENS, HB * THIN_CHANNEL_DIM), 1.0, 6.0, ((0, 8), (1, 4))),
        "slim_lookup_tensor": noise(keys[5], (TOKENS, HB * THIN_CHANNEL_DIM), 1.0, 6.0, ((0, 8), (1, 4))),
        "slim_payload_tensor": noise(keys[6], (TOKENS, HB * THIN_CHANNEL_DIM), 1.0, 6.0, ((0, 8), (1, 4))),
        "slim_emission_valve": noise(keys[7], (TOKENS, HB * THIN_CHANNEL_DIM), 1.0, 6.0, ((0, 8), (1, 4))),
        "broad_forgetting_speed": draw_broad_forgetting_speed(jax.random.fold_in(keys[22], 71), 0),
        "slim_forgetting_speed": draw_slim_forgetting_speed(jax.random.fold_in(keys[22], 71), 0),
        "broad_channel_scaling": jnp.clip(1.0 + 0.18 * jax.random.normal(keys[10], (HA * BROAD_CHANNEL_DIM,), jnp.float32), 0.1, 1.9),
        "slim_channel_scaling": jnp.clip(1.0 + 0.18 * jax.random.normal(keys[11], (HB * THIN_CHANNEL_DIM,), jnp.float32), 0.1, 1.9),
        "surge_forgetting": draw_surge_forgetting(jax.random.fold_in(keys[22], 71), 0),
        "broad_emission_proj": noise(keys[13], (HA * BROAD_CHANNEL_DIM, D), (HA * BROAD_CHANNEL_DIM + HB * THIN_CHANNEL_DIM) ** -0.5, 0.125),
        "slim_emission_proj": noise(keys[14], (HB * THIN_CHANNEL_DIM, D), (HA * BROAD_CHANNEL_DIM + HB * THIN_CHANNEL_DIM) ** -0.5, 0.125),
        "skip_stream": noise(keys[15], (TOKENS, D), 1.0, 6.0, ((0, 32),)),
        "premix_scaling_coeffs": jnp.clip(1.0 + 0.18 * jax.random.normal(keys[16], (D,), jnp.float32), 0.1, 1.9),
        "routed_specialist_ids": draw_routed_specialist_ids(jax.random.fold_in(keys[22], 71), 0),
        "routed_specialist_shares": jnp.clip(0.2 + 0.8 * jax.random.uniform(keys[18], (TOKENS, 2), jnp.float32) ** steps_of(keys[18], (TOKENS, 2), ((0, 8),), -0.2, 0.2), 0.2, 1.0),
        "specialist_valve_proj": noise(keys[19], (EXPERTS, D, FFE), D ** -0.5, 0.125, ((0, 8), (2, 4))),
        "specialist_expand_proj": noise(keys[20], (EXPERTS, D, FFE), D ** -0.5, 0.125, ((0, 8), (2, 4))),
        "specialist_contract_proj": noise(keys[21], (EXPERTS, FFE, D), FFE ** -0.5, 0.125, ((0, 8), (1, 4))),
    }


rope_base = 10000.0
epsilon = 1e-06

def rotate(payload_tensor, positions):
    channel_dimension = payload_tensor.shape[-1]
    half = channel_dimension // 2
    freq = rope_base ** (-jnp.arange(half, dtype=jnp.float32) * 2.0 / channel_dimension)
    angle = positions.astype(jnp.float32)[:, None, None] * freq[None, None, :]
    cosine = jnp.cos(angle)
    sine = jnp.sin(angle)
    first = payload_tensor[..., :half]
    second = payload_tensor[..., half:]
    return jnp.concatenate([first * cosine - second * sine, first * sine + second * cosine], -1)

def prepare(probe_source, lookup_tensor, payload_tensor, heads, channel_dimension):
    length = probe_source.shape[0]
    places = jnp.arange(length, dtype=jnp.int32)
    spun_probe = rotate(probe_source.astype(jnp.float32).reshape(length, heads, channel_dimension), places).astype(jnp.bfloat16)
    spun_lookup = (rotate(lookup_tensor.astype(jnp.float32).reshape(length, heads, channel_dimension), places) * channel_dimension ** (-0.5)).astype(jnp.bfloat16)
    return (spun_probe, spun_lookup, payload_tensor.reshape(length, heads, channel_dimension))

def segment_terms(probe_tensor, lookup_tensor, payload_tensor, surge_forgetting, forgetting_speed):
    length = probe_tensor.shape[0]
    segment_tally = jnp.arange(length, dtype=jnp.float32)
    memory_matrix = forgetting_speed[None, :] * segment_tally[:, None] + jnp.cumsum(surge_forgetting)[:, None]
    causal = (segment_tally[:, None] >= segment_tally[None, :])[None]
    level_t = jnp.transpose(memory_matrix)
    gap = level_t[:, :, None] - level_t[:, None, :]
    decay = jnp.where(causal, jnp.exp(jnp.where(causal, gap, 0.0)), 0.0)
    attention_scores = jnp.einsum('szr,yzr->zsy', probe_tensor.astype(jnp.float32), lookup_tensor.astype(jnp.float32))
    weights = (attention_scores * decay).astype(jnp.bfloat16)
    inner = jnp.einsum('htm,mhe->the', weights.astype(jnp.float32), payload_tensor.astype(jnp.float32))
    factor = jnp.exp(memory_matrix + forgetting_speed[None, :])
    tail = jnp.exp(memory_matrix[-1:, :] - memory_matrix)
    weighted_output = (lookup_tensor.astype(jnp.float32) * tail[:, :, None]).astype(jnp.bfloat16)
    state_update = jnp.einsum('oup,our->upr', weighted_output.astype(jnp.float32), payload_tensor.astype(jnp.float32))
    total = jnp.exp(memory_matrix[-1] + forgetting_speed)
    return (inner, factor, state_update, total)

def read_state(probe_tensor, state):
    return jnp.einsum('thd,hde->the', probe_tensor.astype(jnp.float32), state, precision=lax.Precision.HIGHEST)

def finish(sublayer_final, emission_valve, scaling_coefficients):
    length, heads, channel_dimension = sublayer_final.shape
    normed = sublayer_final * lax.rsqrt(lax.optimization_barrier(jnp.mean(sublayer_final * sublayer_final, -1, keepdims=True)) + epsilon)
    gated = normed.reshape(length, heads * channel_dimension) * scaling_coefficients[None, :] * jax.nn.silu(emission_valve.astype(jnp.float32))
    return gated.astype(jnp.bfloat16)

def keeping_multiplier(probe_source, lookup_tensor, payload_tensor, emission_valve, forgetting_speed, scaling_coefficients, surge_forgetting, channel_dimension):
    heads = probe_source.shape[1] // channel_dimension
    spun_probe, spun_lookup, regrouped_payload = prepare(probe_source, lookup_tensor, payload_tensor, heads, channel_dimension)
    count = TOKENS // BLOCK

    def divider_mark(array):
        return array.reshape((count, BLOCK) + array.shape[1:])

    def segment_walker(state, piece):
        block_q, block_k, block_v, block_b = piece
        inner, factor, state_update, total = segment_terms(block_q, block_k, block_v, block_b, forgetting_speed)
        sublayer_final = inner + factor[:, :, None] * read_state(block_q, state)
        return (total[:, None, None] * state + state_update, sublayer_final)
    opening_location = jnp.zeros((heads, channel_dimension, channel_dimension), jnp.float32)
    ignored_placeholder, sublayer_final = lax.scan(segment_walker, opening_location, (divider_mark(spun_probe), divider_mark(spun_lookup), divider_mark(regrouped_payload), divider_mark(surge_forgetting)))
    return finish(sublayer_final.reshape(TOKENS, heads, channel_dimension), emission_valve, scaling_coefficients)

def experts_mix(normed, routed_specialist_ids, routed_specialist_shares, specialist_valve_proj, specialist_expand_proj, specialist_contract_proj):
    most = N_SP * N_TP * CAP
    slice_width = FFE // N_TP
    padded = jnp.concatenate([normed, jnp.zeros((1, D), jnp.bfloat16)], 0)

    def one(accum, index):
        matches = routed_specialist_ids == index
        weight = lax.optimization_barrier(jnp.sum(jnp.where(matches, routed_specialist_shares, 0.0), 1))
        weight = jnp.concatenate([weight, jnp.zeros((1,), jnp.float32)], 0)
        picked = jnp.nonzero(jnp.any(matches, 1), size=most, fill_value=TOKENS)[0].astype(jnp.int32)
        taken = padded[picked]
        emission_valve = jnp.dot(taken, specialist_valve_proj[index], preferred_element_type=jnp.float32)
        up = jnp.dot(taken, specialist_expand_proj[index], preferred_element_type=jnp.float32)
        hidden = (jax.nn.silu(emission_valve) * up).astype(jnp.bfloat16).reshape(most, N_TP, slice_width)
        down = specialist_contract_proj[index].reshape(N_TP, slice_width, D)
        partial_value = jnp.einsum('mpf,pfd->pmd', hidden.astype(jnp.float32), down.astype(jnp.float32))
        rounded = lax.optimization_barrier(partial_value.astype(jnp.bfloat16))
        expert_out = lax.optimization_barrier(jnp.sum(rounded.astype(jnp.float32), 0)).astype(jnp.bfloat16)
        accum = accum.at[picked].add(weight[picked][:, None] * expert_out.astype(jnp.float32))
        return (accum, None)
    opening_location = jnp.zeros((TOKENS + 1, D), jnp.float32)
    accum, ignored_placeholder = lax.scan(one, opening_location, jnp.arange(EXPERTS, dtype=jnp.int32))
    return accum[:TOKENS]

def reference(broad_probe_tensor, broad_lookup_tensor, broad_payload_tensor, broad_emission_valve, slim_probe_tensor, slim_lookup_tensor, slim_payload_tensor, slim_emission_valve, broad_forgetting_speed, slim_forgetting_speed, broad_channel_scaling, slim_channel_scaling, surge_forgetting, broad_emission_proj, slim_emission_proj, skip_stream, premix_scaling_coeffs, routed_specialist_ids, routed_specialist_shares, specialist_valve_proj, specialist_expand_proj, specialist_contract_proj):
    broad_channel_total = keeping_multiplier(broad_probe_tensor, broad_lookup_tensor, broad_payload_tensor, broad_emission_valve, broad_forgetting_speed, broad_channel_scaling, surge_forgetting, BROAD_CHANNEL_DIM)
    slim_channel_total = keeping_multiplier(slim_probe_tensor, slim_lookup_tensor, slim_payload_tensor, slim_emission_valve, slim_forgetting_speed, slim_channel_scaling, surge_forgetting, THIN_CHANNEL_DIM)
    projected = jnp.dot(broad_channel_total, broad_emission_proj, preferred_element_type=jnp.float32)
    projected = projected + jnp.dot(slim_channel_total, slim_emission_proj, preferred_element_type=jnp.float32)
    updated = skip_stream.astype(jnp.float32) + projected
    scale = lax.rsqrt(lax.optimization_barrier(jnp.mean(updated * updated, -1, keepdims=True)) + epsilon)
    normed = (updated * scale * premix_scaling_coeffs[None, :]).astype(jnp.bfloat16)
    mixture = experts_mix(normed, routed_specialist_ids, routed_specialist_shares, specialist_valve_proj, specialist_expand_proj, specialist_contract_proj)
    return (updated + mixture).astype(jnp.bfloat16)
```

```python
import jax
import jax.numpy as jnp
from jax import lax
from jax.experimental import pallas as pl
from jax.experimental.pallas import tpu as pltpu
from jax.sharding import PartitionSpec as P

MESH = pl.DeviceIdType.MESH
VMEM_SPEC = pl.BlockSpec(memory_space=pltpu.VMEM)

BROAD_CHANNEL_DIM = 128
THIN_CHANNEL_DIM = 64
GROUPS = 4


rope_base = 10000.0
epsilon = 1e-06


def exchange_kernel(state_ref, tile_ref, states_ref, tiles_ref, send_sem, recv_sem):
    me = lax.axis_index("sp")
    count = states_ref.shape[0]
    barrier = pltpu.get_barrier_semaphore()
    for step in range(1, count):
        pl.semaphore_signal(
            barrier, inc=1, device_id={"sp": lax.rem(me + step, count)}, device_id_type=MESH
        )
    pl.semaphore_wait(barrier, count - 1)
    copies = []
    for step in range(1, count):
        for kind, (src, dst) in enumerate(((state_ref, states_ref), (tile_ref, tiles_ref))):
            copy = pltpu.make_async_remote_copy(
                src_ref=src,
                dst_ref=dst.at[me],
                send_sem=send_sem.at[kind, step],
                recv_sem=recv_sem.at[kind, step],
                device_id={"sp": lax.rem(me + step, count)},
                device_id_type=MESH,
            )
            copy.start()
            copies.append(copy)
    states_ref[me] = state_ref[...]
    tiles_ref[me] = tile_ref[...]
    for copy in copies:
        copy.wait()


def exchange(state, tile):
    count = lax.axis_size("sp")
    return pl.pallas_call(
        exchange_kernel,
        out_shape=(
            jax.ShapeDtypeStruct((count,) + state.shape, state.dtype),
            jax.ShapeDtypeStruct((count,) + tile.shape, tile.dtype),
        ),
        in_specs=[VMEM_SPEC] * 2,
        out_specs=(VMEM_SPEC, VMEM_SPEC),
        scratch_shapes=[
            pltpu.SemaphoreType.DMA((2, count)),
            pltpu.SemaphoreType.DMA((2, count)),
        ],
        compiler_params=pltpu.CompilerParams(collective_id=0, has_side_effects=True),
        name="state_exchange",
    )(state, tile)


def places_of(groups):
    sp = lax.axis_index("sp")
    tp = lax.axis_index("tp")
    core = lax.rem(tp, 2)
    x = lax.rem(sp, 2)
    y = tp // 2
    across_sp = sp + 1 - 2 * x
    across_tp = tp + 2 - 4 * y
    near = {"sp": across_sp + core * (sp - across_sp), "tp": tp + core * (across_tp - tp)}
    side = {"sp": sp + core * (across_sp - sp), "tp": across_tp + core * (tp - across_tp)}
    twin = {"sp": sp, "tp": tp + 1 - 2 * core}
    group = sp // 2
    far = [{"sp": lax.rem(group + step, groups) * 2 + x, "tp": tp} for step in range(groups)]
    return group, x, y, core, near, side, twin, far


def experts_kernel(
    rows_ref,
    shares_ref,
    valve_ref,
    expand_ref,
    contract_ref,
    out_ref,
    slots,
    valve,
    expand,
    contract,
    hidden,
    kept,
    leave,
    landed,
    joined,
    met,
    back,
    load_sem,
    swap_send,
    swap_recv,
    far_send,
    far_recv,
    near_send,
    near_recv,
    fold_send,
    fold_recv,
    home_send,
    home_recv,
):
    groups, cap, width = rows_ref.shape
    units = valve_ref.shape[1]
    group, x, y, core, near, side, twin, far = places_of(groups)
    barrier = pltpu.get_barrier_semaphore()
    friends = [near, side, twin] + far[1:]
    for friend in friends:
        pl.semaphore_signal(barrier, inc=1, device_id=friend, device_id_type=MESH)
    pl.semaphore_wait(barrier, len(friends))
    sent = []

    def send(src, dst, send_sem, recv_sem, device):
        copy = pltpu.make_async_remote_copy(
            src_ref=src,
            dst_ref=dst,
            send_sem=send_sem,
            recv_sem=recv_sem,
            device_id=device,
            device_id_type=MESH,
        )
        copy.start()
        sent.append(copy)
        return copy

    order = [0, 1, 3, 2]
    arriving = {}
    for step in order[1:]:
        arriving[step] = send(
            rows_ref.at[lax.rem(group + step, groups)],
            slots.at[step, 0],
            far_send.at[step],
            far_recv.at[step],
            far[step],
        )
    own = {}

    def spread(step):
        if step > 0:
            arriving[step].wait_recv()
        src = rows_ref.at[group] if step == 0 else slots.at[step, 0]
        own[step] = [
            send(src, slots.at[step, 1], near_send.at[step, 0], near_recv.at[step, 0], near),
            send(src, slots.at[step, 2], near_send.at[step, 1], near_recv.at[step, 1], side),
        ]

    def forward(step):
        own[step][0].wait_recv()
        own[step].append(
            send(
                slots.at[step, 1],
                slots.at[step, 3],
                near_send.at[step, 2],
                near_recv.at[step, 2],
                side,
            )
        )

    spread(0)
    loads = []
    swaps = []
    for index, (src, dst) in enumerate(
        ((valve_ref, valve), (expand_ref, expand), (contract_ref, contract))
    ):
        load = pltpu.make_async_copy(src, dst.at[core], load_sem.at[index])
        load.start()
        loads.append(load)
        swaps.append(send(src, dst.at[core], swap_send.at[index], swap_recv.at[index], twin))
    slots[0, 0] = rows_ref[group]
    forward(0)
    spread(order[1])

    def shares_for(step):
        origin = lax.rem(group + groups - step, groups)
        near_x = 1 - x + core * (2 * x - 1)
        near_y = y + core * (1 - 2 * y)
        return jnp.concatenate(
            [
                shares_ref[origin, x, y],
                shares_ref[origin, near_x, near_y],
                shares_ref[origin, 1 - near_x + 0 * x, 1 - near_y],
                shares_ref[origin, 1 - x, 1 - y],
            ],
            0,
        )

    tile = 256
    across = 512

    def widen(step):
        share = shares_for(step)
        batch = slots[step].reshape(4 * cap, width)

        def one(index, carry):
            half = index // (units // tile)
            begin = pl.multiple_of(lax.rem(index, units // tile) * tile, tile)
            gate = jnp.dot(
                batch, valve[half, :, pl.ds(begin, tile)], preferred_element_type=jnp.float32
            )
            up = jnp.dot(
                batch, expand[half, :, pl.ds(begin, tile)], preferred_element_type=jnp.float32
            )
            place = pl.multiple_of(index * tile, tile)
            hidden[:, pl.ds(place, tile)] = (jax.nn.silu(gate) * up * share).astype(hidden.dtype)
            return carry

        lax.fori_loop(0, 2 * units // tile, one, 0)

    def narrow(step):
        def one(index, carry):
            begin = pl.multiple_of(index * across, across)
            column = pl.ds(begin, across)
            part = jnp.dot(
                hidden[:, :units], contract[0, :, column], preferred_element_type=jnp.float32
            ) + jnp.dot(
                hidden[:, units:], contract[1, :, column], preferred_element_type=jnp.float32
            )
            kept[step, :, :, column] = part[: 2 * cap].reshape(2, cap, across)
            leave[step, :, :, column] = part[2 * cap :].reshape(2, cap, across).astype(leave.dtype)
            return carry

        lax.fori_loop(0, width // across, one, 0)
        folding[step] = send(
            leave.at[step], landed.at[step], fold_send.at[step, 0], fold_recv.at[step, 0], side
        )

    folding = {}
    joining = {}

    def join(step):
        folding[step].wait_recv()
        joined[step] = (kept[step, 1] + landed[step, 1].astype(jnp.float32)).astype(joined.dtype)
        joining[step] = send(
            joined.at[step], met.at[step], fold_send.at[step, 1], fold_recv.at[step, 1], near
        )
        kept[step, 0] = kept[step, 0] + landed[step, 0].astype(jnp.float32)

    homing = []

    def finish_step(step):
        joining[step].wait_recv()
        total = (kept[step, 0] + met[step].astype(jnp.float32)).astype(out_ref.dtype)
        if step == 0:
            out_ref[group] = total
        else:
            back[step] = total
            homing.append(
                send(
                    back.at[step],
                    out_ref.at[group],
                    home_send.at[step],
                    home_recv.at[step],
                    far[groups - step],
                )
            )

    for place, step in enumerate(order):
        own[step][1].wait_recv()
        own[step][2].wait_recv()
        if place == 0:
            for load, swap in zip(loads, swaps):
                load.wait()
                swap.wait_recv()
        widen(step)
        if place + 1 < groups:
            forward(order[place + 1])
        if place + 2 < groups:
            spread(order[place + 2])
        narrow(step)
        if place >= 1:
            join(order[place - 1])
        if place >= 2:
            finish_step(order[place - 2])
    join(order[-1])
    finish_step(order[-2])
    finish_step(order[-1])
    for copy in homing:
        copy.wait_recv()
    for copy in sent:
        copy.wait_send()


def experts_plane(rows, shares, valve, expand, contract):
    groups, cap, width = rows.shape
    units = valve.shape[1]
    kind = rows.dtype
    any_spec = pl.BlockSpec(memory_space=pl.ANY)
    dma = pltpu.SemaphoreType.DMA
    return pl.pallas_call(
        experts_kernel,
        out_shape=jax.ShapeDtypeStruct(rows.shape, kind),
        in_specs=[VMEM_SPEC] * 2 + [any_spec] * 3,
        out_specs=VMEM_SPEC,
        scratch_shapes=[
            pltpu.VMEM((groups, 4, cap, width), kind),
            pltpu.VMEM((2,) + valve.shape, kind),
            pltpu.VMEM((2,) + expand.shape, kind),
            pltpu.VMEM((2,) + contract.shape, kind),
            pltpu.VMEM((4 * cap, 2 * units), kind),
            pltpu.VMEM((groups, 2, cap, width), jnp.float32),
            pltpu.VMEM((groups, 2, cap, width), kind),
            pltpu.VMEM((groups, 2, cap, width), kind),
            pltpu.VMEM((groups, cap, width), kind),
            pltpu.VMEM((groups, cap, width), kind),
            pltpu.VMEM((groups, cap, width), kind),
            dma((3,)),
            dma((3,)),
            dma((3,)),
            dma((groups,)),
            dma((groups,)),
            dma((groups, 3)),
            dma((groups, 3)),
            dma((groups, 2)),
            dma((groups, 2)),
            dma((groups,)),
            dma((groups,)),
        ],
        compiler_params=pltpu.CompilerParams(
            collective_id=3, has_side_effects=True, vmem_limit_bytes=56 * 1024 * 1024
        ),
        name="experts_plane",
    )(rows, shares, valve, expand, contract)


def rotate(payload_tensor, positions):
    channel_dimension = payload_tensor.shape[-1]
    half = channel_dimension // 2
    freq = rope_base ** (-jnp.arange(half, dtype=jnp.float32) * 2.0 / channel_dimension)
    angle = positions.astype(jnp.float32)[:, None, None] * freq[None, None, :]
    cosine = jnp.cos(angle)
    sine = jnp.sin(angle)
    first = payload_tensor[..., :half]
    second = payload_tensor[..., half:]
    return jnp.concatenate([first * cosine - second * sine, first * sine + second * cosine], -1)


def segment_terms(probe_tensor, lookup_tensor, payload_tensor, surge_forgetting, forgetting_speed):
    length = probe_tensor.shape[0]
    segment_tally = jnp.arange(length, dtype=jnp.float32)
    memory_matrix = (
        forgetting_speed[None, :] * segment_tally[:, None] + jnp.cumsum(surge_forgetting)[:, None]
    )
    causal = (segment_tally[:, None] >= segment_tally[None, :])[None]
    level_t = jnp.transpose(memory_matrix)
    gap = level_t[:, :, None] - level_t[:, None, :]
    decay = jnp.where(causal, jnp.exp(jnp.where(causal, gap, 0.0)), 0.0)
    attention_scores = jnp.einsum(
        "szr,yzr->zsy", probe_tensor, lookup_tensor, preferred_element_type=jnp.float32
    )
    weights = (attention_scores * decay).astype(jnp.bfloat16)
    inner = jnp.einsum("htm,mhe->the", weights, payload_tensor, preferred_element_type=jnp.float32)
    factor = jnp.exp(memory_matrix + forgetting_speed[None, :])
    tail = jnp.exp(memory_matrix[-1:, :] - memory_matrix)
    weighted_output = (lookup_tensor.astype(jnp.float32) * tail[:, :, None]).astype(jnp.bfloat16)
    state_update = jnp.einsum(
        "oup,our->upr", weighted_output, payload_tensor, preferred_element_type=jnp.float32
    )
    total = memory_matrix[-1] + forgetting_speed
    return (inner, factor, state_update, total)


def read_state(probe_tensor, state):
    return jnp.einsum(
        "thd,hde->the", probe_tensor.astype(jnp.float32), state, precision=lax.Precision.HIGHEST
    )


def keeping_multiplier(
    probe_source,
    lookup_tensor,
    payload_tensor,
    forgetting_speed,
    surge_forgetting,
    channel_dimension,
    segment_begin,
):
    length = probe_source.shape[0]
    heads = probe_source.shape[1] // channel_dimension
    places = segment_begin + jnp.arange(length, dtype=jnp.int32)
    spun_probe = rotate(
        probe_source.astype(jnp.float32).reshape(length, heads, channel_dimension), places
    ).astype(jnp.bfloat16)
    spun_lookup = (
        rotate(lookup_tensor.astype(jnp.float32).reshape(length, heads, channel_dimension), places)
        * channel_dimension ** (-0.5)
    ).astype(jnp.bfloat16)
    regrouped_payload = payload_tensor.reshape(length, heads, channel_dimension)
    block = min(512, length)
    count = length // block

    def divider_mark(array):
        return array.reshape((count, block) + array.shape[1:])

    state, level, local, reach = None, None, [], []
    for piece in zip(
        divider_mark(spun_probe),
        divider_mark(spun_lookup),
        divider_mark(regrouped_payload),
        divider_mark(surge_forgetting),
    ):
        inner, factor, state_update, total = segment_terms(*piece, forgetting_speed)
        if state is None:
            state, level = state_update, total
        else:
            inner = inner + factor[:, :, None] * read_state(piece[0], state)
            factor = factor * jnp.exp(level)[None, :]
            state, level = jnp.exp(total)[:, None, None] * state + state_update, level + total
        local.append(inner)
        reach.append(factor)
    return (
        spun_probe,
        jnp.concatenate(local, 0),
        jnp.concatenate(reach, 0),
        level,
        state,
    )


def finish(sublayer_final, emission_valve, scaling_coefficients):
    length, heads, channel_dimension = sublayer_final.shape
    normed = sublayer_final * lax.rsqrt(
        jnp.mean(sublayer_final * sublayer_final, -1, keepdims=True) + epsilon
    )
    gated = (
        normed.reshape(length, heads * channel_dimension)
        * scaling_coefficients[None, :]
        * jax.nn.silu(emission_valve.astype(jnp.float32))
    )
    return gated.astype(jnp.bfloat16)


def carried(states, levels):
    place = lax.axis_index("sp")
    count = states.shape[0]
    index = jnp.arange(count, dtype=jnp.int32)
    between = (index[None, :] > index[:, None]) & (index[None, :] < place)
    reach = jnp.sum(jnp.where(between[:, :, None], levels[None, :, :], 0.0), 1)
    weight = jnp.where((index < place)[:, None], jnp.exp(reach), 0.0)
    return jnp.sum(weight[:, :, None, None] * states.astype(jnp.float32), 0)


def slot_positions(chosen, experts, cap):
    listed = chosen.reshape(-1)
    matches = (listed[:, None] == jnp.arange(experts, dtype=jnp.int32)[None, :]).astype(jnp.int32)
    before = jnp.cumsum(matches, 0) - matches
    order = jnp.sum(before * matches, 1)
    return (listed * cap + order).reshape(chosen.shape)


def fill_slots(rows_in, chosen, experts, cap):
    count = rows_in.shape[0]
    places = slot_positions(chosen, experts, cap).reshape(-1)
    owners = jnp.repeat(jnp.arange(count, dtype=jnp.int32), 2)
    source = jnp.full((experts * cap,), count, jnp.int32).at[places].set(owners)
    padded = jnp.concatenate([rows_in, jnp.zeros((1, rows_in.shape[1]), rows_in.dtype)], 0)
    return padded[source].reshape(experts, cap, rows_in.shape[1])


def shares_by_slot(ids, shares, rows, cap):
    core = lax.rem(lax.axis_index("tp"), 2)
    ids = lax.dynamic_index_in_dim(ids.reshape(-1, 2, rows, 2), core, 1, False)
    shares = lax.dynamic_index_in_dim(shares.reshape(-1, 2, rows, 2), core, 1, False)
    group = ids[:, :, 0] // 2
    named = group[:, :, None] == jnp.arange(GROUPS, dtype=jnp.int32)
    rank = jnp.cumsum(named.astype(jnp.int32), 1) - 1
    slot = group * cap + jnp.sum(jnp.where(named, rank, 0), 2)
    holds = slot[:, None, :] == jnp.arange(GROUPS * cap, dtype=jnp.int32)[None, :, None]
    found = []
    for member in range(2):
        share = jnp.sum(jnp.where(ids - 2 * group[:, :, None] == member, shares, 0.0), 2)
        found.append(jnp.sum(jnp.where(holds, share[:, None, :], 0.0), 2))
    return jnp.stack(found, 1).reshape(-1)


def on_device(
    broad_probe_tensor,
    broad_lookup_tensor,
    broad_payload_tensor,
    broad_emission_valve,
    slim_probe_tensor,
    slim_lookup_tensor,
    slim_payload_tensor,
    slim_emission_valve,
    broad_forgetting_speed,
    slim_forgetting_speed,
    broad_channel_scaling,
    slim_channel_scaling,
    surge_forgetting,
    broad_emission_proj,
    slim_emission_proj,
    skip_stream,
    premix_scaling_coeffs,
    routed_specialist_ids,
    routed_specialist_shares,
    specialist_valve_proj,
    specialist_expand_proj,
    specialist_contract_proj,
):
    length = broad_probe_tensor.shape[0]
    segment_begin = lax.axis_index("sp") * length
    plane = lax.axis_size("sp") * specialist_valve_proj.shape[0] == 2 * GROUPS and (
        lax.axis_size("tp") == 4
    )
    if not plane:
        valve_all = lax.all_gather(specialist_valve_proj[0], "tp")
        expand_all = lax.all_gather(specialist_expand_proj[0], "tp")
        contract_all = lax.all_gather(specialist_contract_proj[0], "tp")
    wide_result = keeping_multiplier(
        broad_probe_tensor,
        broad_lookup_tensor,
        broad_payload_tensor,
        broad_forgetting_speed,
        surge_forgetting,
        BROAD_CHANNEL_DIM,
        segment_begin,
    )
    narrow_result = keeping_multiplier(
        slim_probe_tensor,
        slim_lookup_tensor,
        slim_payload_tensor,
        slim_forgetting_speed,
        surge_forgetting,
        THIN_CHANNEL_DIM,
        segment_begin,
    )
    rows = skip_stream.shape[0]
    width = skip_stream.shape[1]
    experts = lax.axis_size("sp") * specialist_valve_proj.shape[0]
    cap = rows * GROUPS // experts
    pair = experts // GROUPS
    own_ids = lax.dynamic_slice_in_dim(routed_specialist_ids, lax.axis_index("tp") * rows, rows, 0)
    own_weights = lax.dynamic_slice_in_dim(
        routed_specialist_shares, lax.axis_index("tp") * rows, rows, 0
    )
    levels = jnp.concatenate([wide_result[3], narrow_result[3]])
    tile = levels
    if plane:
        group_of = own_ids[:, 0] // pair
        named = group_of[:, None] == jnp.arange(GROUPS, dtype=jnp.int32)[None, :]
        rank = jnp.cumsum(named.astype(jnp.int32), 0) - 1
        own_slot = group_of * cap + jnp.sum(jnp.where(named, rank, 0), 1)
        holds = own_slot[None, :] == jnp.arange(GROUPS * cap, dtype=jnp.int32)[:, None]
        tile = jnp.concatenate(
            [levels, shares_by_slot(routed_specialist_ids, routed_specialist_shares, rows, cap)]
        )
    tile_size = -(-tile.shape[0] // 1024) * 1024
    tile = jnp.pad(tile, (0, tile_size - tile.shape[0])).reshape(-1, 128)
    packed = jnp.concatenate(
        [wide_result[4].reshape(-1, 128), narrow_result[4].reshape(-1, 128)], 0
    ).astype(jnp.bfloat16)
    states, tiles = exchange(packed, tile)
    count = states.shape[0]
    tiles = tiles.reshape(count, -1)
    wide_heads = wide_result[3].shape[0]
    both_heads = levels.shape[0]
    cut = wide_result[4].size // 128
    incoming_wide = carried(
        states[:, :cut].reshape((count,) + wide_result[4].shape), tiles[:, :wide_heads]
    )
    incoming_narrow = carried(
        states[:, cut:].reshape((count,) + narrow_result[4].shape),
        tiles[:, wide_heads:both_heads],
    )
    mixed_wide = finish(
        wide_result[1] + wide_result[2][:, :, None] * read_state(wide_result[0], incoming_wide),
        broad_emission_valve,
        broad_channel_scaling,
    )
    mixed_narrow = finish(
        narrow_result[1] + narrow_result[2][:, :, None] * read_state(narrow_result[0], incoming_narrow),
        slim_emission_valve,
        slim_channel_scaling,
    )
    rows_wide, rows_narrow = (
        lax.all_to_all(mixed_wide, "tp", split_axis=0, concat_axis=1, tiled=True),
        lax.all_to_all(mixed_narrow, "tp", split_axis=0, concat_axis=1, tiled=True),
    )
    projected = jnp.dot(rows_wide, broad_emission_proj, preferred_element_type=jnp.float32)
    projected = projected + jnp.dot(
        rows_narrow, slim_emission_proj, preferred_element_type=jnp.float32
    )
    updated = skip_stream.astype(jnp.float32) + projected
    scale = lax.rsqrt(jnp.mean(updated * updated, -1, keepdims=True) + epsilon)
    normed = (updated * scale * premix_scaling_coeffs[None, :]).astype(jnp.bfloat16)
    if plane:
        spread = holds.astype(jnp.bfloat16)
        filled = jnp.dot(spread, normed, preferred_element_type=jnp.float32).astype(jnp.bfloat16)
        shares = tiles[:, both_heads : both_heads + 4 * GROUPS * cap]
        shares = shares.reshape(GROUPS, 2, 2, 2, GROUPS, cap)
        place = lax.axis_index("sp")
        shares = lax.dynamic_index_in_dim(shares, place % 2, 3, False)
        shares = lax.dynamic_index_in_dim(shares, place // 2, 3, False)
        returned = experts_plane(
            filled.reshape(GROUPS, cap, width),
            shares[..., None],
            specialist_valve_proj[0],
            specialist_expand_proj[0],
            specialist_contract_proj[0],
        ).reshape(-1, width)
        mixture = lax.dot_general(
            spread, returned, (((0,), (0,)), ((), ())), preferred_element_type=jnp.float32
        )
        return (updated + mixture).astype(jnp.bfloat16)
    own_places = slot_positions(own_ids, experts, cap)
    slots = lax.all_to_all(
        fill_slots(normed, own_ids, experts, cap), "sp", split_axis=0, concat_axis=0, tiled=True
    ).reshape(-1, width)
    expert_out = None
    for part in range(lax.axis_size("tp")):
        emission_valve = jnp.dot(slots, valve_all[part], preferred_element_type=jnp.float32)
        up = jnp.dot(slots, expand_all[part], preferred_element_type=jnp.float32)
        hidden = (jax.nn.silu(emission_valve) * up).astype(jnp.bfloat16)
        term = jnp.dot(hidden, contract_all[part], preferred_element_type=jnp.float32)
        expert_out = term if expert_out is None else expert_out + term
    returned = lax.all_to_all(
        expert_out.astype(jnp.bfloat16).reshape(experts, cap, width),
        "sp",
        split_axis=0,
        concat_axis=0,
        tiled=True,
    )
    picked = returned.reshape(experts * cap, width)[own_places]
    mixture = jnp.sum(own_weights[:, :, None] * picked.astype(jnp.float32), 1)
    return (updated + mixture).astype(jnp.bfloat16)


def solution(mesh):
    return jax.shard_map(
        on_device,
        mesh=mesh,
        in_specs=(
            P("sp", "tp"),
            P("sp", "tp"),
            P("sp", "tp"),
            P("sp", "tp"),
            P("sp", "tp"),
            P("sp", "tp"),
            P("sp", "tp"),
            P("sp", "tp"),
            P("tp"),
            P("tp"),
            P("tp"),
            P("tp"),
            P("sp"),
            P(),
            P(),
            P(("sp", "tp"), None),
            P(),
            P("sp", None),
            P("sp", None),
            P("sp", None, "tp"),
            P("sp", None, "tp"),
            P("sp", "tp", None),
        ),
        out_specs=P(("sp", "tp"), None),
        check_vma=False,
    )
```

```python
import jax
import jax.numpy as jnp
import numpy as np
from jax import lax
from jax.experimental import pallas as pl
from jax.experimental.pallas import tpu as pltpu
from jax.sharding import PartitionSpec as P

MESH = pl.DeviceIdType.MESH
VMEM_SPEC = pl.BlockSpec(memory_space=pltpu.VMEM)

BROAD_CHANNEL_DIM = 128
THIN_CHANNEL_DIM = 64
GROUPS = 4


rope_base = 10000.0
epsilon = 1e-06


def exchange_kernel(state_ref, tile_ref, states_ref, tiles_ref, send_sem, recv_sem):
    me = lax.axis_index("sp")
    count = states_ref.shape[0]
    barrier = pltpu.get_barrier_semaphore()
    for step in range(1, count):
        pl.semaphore_signal(
            barrier, inc=1, device_id={"sp": lax.rem(me + step, count)}, device_id_type=MESH
        )
    pl.semaphore_wait(barrier, count - 1)
    copies = []
    for step in range(1, count):
        for kind, (src, dst) in enumerate(((state_ref, states_ref), (tile_ref, tiles_ref))):
            copy = pltpu.make_async_remote_copy(
                src_ref=src,
                dst_ref=dst.at[me],
                send_sem=send_sem.at[kind, step],
                recv_sem=recv_sem.at[kind, step],
                device_id={"sp": lax.rem(me + step, count)},
                device_id_type=MESH,
            )
            copy.start()
            copies.append(copy)
    states_ref[me] = state_ref[...]
    tiles_ref[me] = tile_ref[...]
    for copy in copies:
        copy.wait()


def exchange(state, tile):
    count = lax.axis_size("sp")
    return pl.pallas_call(
        exchange_kernel,
        out_shape=(
            jax.ShapeDtypeStruct((count,) + state.shape, state.dtype),
            jax.ShapeDtypeStruct((count,) + tile.shape, tile.dtype),
        ),
        in_specs=[VMEM_SPEC] * 2,
        out_specs=(VMEM_SPEC, VMEM_SPEC),
        scratch_shapes=[
            pltpu.SemaphoreType.DMA((2, count)),
            pltpu.SemaphoreType.DMA((2, count)),
        ],
        compiler_params=pltpu.CompilerParams(collective_id=0, has_side_effects=True),
        name="state_exchange",
    )(state, tile)


def places_of(groups):
    sp = lax.axis_index("sp")
    tp = lax.axis_index("tp")
    core = lax.rem(tp, 2)
    x = lax.rem(sp, 2)
    y = tp // 2
    across_sp = sp + 1 - 2 * x
    across_tp = tp + 2 - 4 * y
    near = {"sp": across_sp + core * (sp - across_sp), "tp": tp + core * (across_tp - tp)}
    side = {"sp": sp + core * (across_sp - sp), "tp": across_tp + core * (tp - across_tp)}
    twin = {"sp": sp, "tp": tp + 1 - 2 * core}
    group = sp // 2
    far = [{"sp": lax.rem(group + step, groups) * 2 + x, "tp": tp} for step in range(groups)]
    return group, x, y, core, near, side, twin, far


def layer_kernel(
    inputs,
    tables_ref,
    turn_ref,
    surge_ref,
    wide_rate,
    slim_rate,
    wide_gain,
    slim_gain,
    wide_proj,
    slim_proj,
    skip_ref,
    premix_ref,
    ids_ref,
    share_ref,
    valve_ref,
    expand_ref,
    contract_ref,
    out_ref,
    staged,
    tables,
    proj,
    skip,
    queries,
    keys,
    faded,
    level,
    inner,
    gates,
    grown,
    grown_out,
    grown_in,
    tile_out,
    tiles,
    plane_out,
    plane_in,
    carry_out,
    carry_in,
    mixed_out,
    mixed,
    updated,
    normed,
    holds,
    rows,
    returned,
    slots,
    valve,
    expand,
    contract,
    hidden,
    kept,
    leave,
    landed,
    joined,
    met,
    back,
    load_sem,
    swap_send,
    swap_recv,
    tile_send,
    tile_recv,
    grown_send,
    grown_recv,
    plane_send,
    plane_recv,
    carry_send,
    carry_recv,
    mixed_send,
    mixed_recv,
    far_send,
    far_recv,
    near_send,
    near_recv,
    fold_send,
    fold_recv,
    home_send,
    home_recv,
):
    f32 = jnp.float32
    bf16 = jnp.bfloat16
    groups, cap, width = rows.shape
    units = valve_ref.shape[1]
    length = staged.shape[1]
    part = skip.shape[0]
    lanes = 128
    blocks = length // part
    count = tiles.shape[0]
    sp = lax.axis_index("sp")
    tp = lax.axis_index("tp")
    group, x, y, core, near, side, twin, far = places_of(groups)
    partner = sp + 1 - 2 * x
    across = tp + 2 - 4 * y
    twin_tp = tp + 1 - 2 * core
    across_twin = twin_tp + 2 - 4 * y

    loads = {}

    def load(name, src, dst):
        copy = pltpu.make_async_copy(src, dst, load_sem.at[len(loads)])
        copy.start()
        loads[name] = copy

    for index in (1, 5):
        load(index, inputs[index], staged.at[index])
    load("tables", tables_ref, tables)
    for index in (2, 6, 0, 4, 3, 7):
        load(index, inputs[index], staged.at[index])
    load("skip", skip_ref, skip)

    barrier = pltpu.get_barrier_semaphore()
    friends = [{"sp": lax.rem(sp + step, count), "tp": tp} for step in range(1, count)]
    friends += [{"sp": sp, "tp": other} for other in (across, twin_tp, across_twin)]
    for friend in friends:
        pl.semaphore_signal(barrier, inc=1, device_id=friend, device_id_type=MESH)
    pl.semaphore_wait(barrier, len(friends))
    sent = []

    def send(src, dst, send_sem, recv_sem, device):
        copy = pltpu.make_async_remote_copy(
            src_ref=src,
            dst_ref=dst,
            send_sem=send_sem,
            recv_sem=recv_sem,
            device_id=device,
            device_id_type=MESH,
        )
        copy.start()
        sent.append(copy)
        return copy

    def iota(shape, axis):
        return lax.broadcasted_iota(jnp.int32, shape, axis)

    lane = iota((part, lanes), 1)
    row = iota((part, lanes), 0)
    eye = lane == row
    low_lane = iota((1, lanes), 1) < lanes // 2

    surge = surge_ref[...]
    wide_lane = iota((part, length), 1)
    wide_row = iota((part, length), 0)
    lines = []
    for block in range(blocks):
        column = jnp.sum(
            jnp.where(wide_lane <= wide_row + block * part, surge, 0.0), 1, keepdims=True
        )
        level[pl.ds(block * part, part), :] = jnp.broadcast_to(column, (part, lanes))
        lines.append(jnp.sum(jnp.where(eye, column, 0.0), 0, keepdims=True))
    surge_line = jnp.concatenate(lines, 1)
    surge_total = jnp.broadcast_to(jnp.sum(surge, 1, keepdims=True), (1, lanes))

    rates = [
        jnp.full((1, lanes), wide_rate[0], f32),
        jnp.full((1, lanes), wide_rate[1], f32),
        jnp.where(low_lane, slim_rate[0], slim_rate[1]),
        jnp.where(low_lane, slim_rate[2], slim_rate[3]),
    ]

    def route(block):
        begin = pl.multiple_of(block * part, part)
        ids = ids_ref[pl.ds(begin, part), :]
        weights = share_ref[pl.ds(begin, part), :]
        first = ids[:, 0:1]
        chosen = lax.shift_right_logical(first, 1)
        named = chosen == lane
        rank = jnp.dot(
            jnp.where(row >= lane, 1.0, 0.0).astype(bf16),
            jnp.where(named, 1.0, 0.0).astype(bf16),
            preferred_element_type=f32,
        )
        order_in = jnp.sum(jnp.where(named, rank, 0.0), 1, keepdims=True).astype(jnp.int32) - 1
        even = first - 2 * chosen == 0
        shares = [
            jnp.where(even, weights[:, 0:1], weights[:, 1:2]),
            jnp.where(even, weights[:, 1:2], weights[:, 0:1]),
        ]
        return chosen, order_in, shares

    chosen, order_in, _ = route(tp)
    holds[...] = jnp.where(
        chosen * cap + order_in == iota((part, groups * cap), 1), 1.0, 0.0
    ).astype(bf16)
    share_lines = [0.0, 0.0]
    for block_y in range(2):
        chosen, order_in, shares = route(2 * block_y + core)
        here = chosen * (2 * cap) + block_y * cap + order_in == iota((part, 2 * groups * cap), 1)
        for member in range(2):
            share_lines[member] = share_lines[member] + jnp.sum(
                jnp.where(here, shares[member], 0.0), 0, keepdims=True
            )
    top = iota((8, lanes), 0) == 0
    for target in range(count):
        line = share_lines[target % 2][:, (target // 2) * lanes : (target // 2 + 1) * lanes]
        tile_out[target] = jnp.where(top, line, surge_total)
    tile_copies = []
    for step in range(1, count):
        other = lax.rem(sp + step, count)
        tile_copies.append(
            send(
                tile_out.at[other],
                tiles.at[sp],
                tile_send.at[step],
                tile_recv.at[step],
                {"sp": other, "tp": tp},
            )
        )
    tiles[sp] = tile_out[sp]

    def turner(size):
        half = size // 2
        low = lax.rem(lane, size) < half
        match = row == jnp.where(low, lane + half, lane - half)
        return jnp.where(match, jnp.where(low, -1.0, 1.0), 0.0).astype(bf16)

    turns = [turner(BROAD_CHANNEL_DIM), turner(THIN_CHANNEL_DIM)]
    scales = [BROAD_CHANNEL_DIM ** (-0.5), THIN_CHANNEL_DIM ** (-0.5)]
    turn = turn_ref[sp]

    def unit_of(index):
        return index // 2, (index % 2) * lanes

    loads["tables"].wait()
    loads[1].wait()
    loads[5].wait()
    last = [rates[unit] * (length - 1) + surge_total for unit in range(4)]

    def turn_keys(block, carry):
        here = pl.ds(pl.multiple_of(block * part, part), part)
        moment = (row + block * part).astype(f32)
        summed = level[here, :]
        for kind in range(2):
            cosine_near = tables[2 * kind, here, :]
            sine_near = tables[2 * kind + 1, here, :]
            cosine_far = turn[2 * kind : 2 * kind + 1]
            sine_far = turn[2 * kind + 1 : 2 * kind + 2]
            cosine = cosine_near * cosine_far - sine_near * sine_far
            sine = sine_near * cosine_far + cosine_near * sine_far
            tables[2 * kind, here, :] = cosine
            tables[2 * kind + 1, here, :] = sine
            for index in range(2):
                unit = 2 * kind + index
                piece = staged[4 * kind + 1, here, index * lanes : (index + 1) * lanes]
                turned = jnp.dot(piece, turns[kind], preferred_element_type=f32)
                key = (
                    (piece.astype(f32) * cosine + turned * sine) * scales[kind]
                ).astype(bf16)
                keys[unit, here, :] = key
                tail = jnp.exp(last[unit] - (rates[unit] * moment + summed))
                faded[unit, here, :] = (key.astype(f32) * tail).astype(bf16)
        return carry

    lax.fori_loop(0, blocks, turn_keys, 0)
    loads[2].wait()
    loads[6].wait()
    for unit in range(4):
        kind, begin = unit_of(unit)
        change = lax.dot_general(
            faded[unit],
            staged[4 * kind + 2, :, begin : begin + lanes],
            (((0,), (0,)), ((), ())),
            preferred_element_type=f32,
        )
        half = unit % 2
        if kind == 0:
            grown[half, :lanes, :] = change
            grown_out[half, :lanes, :] = change.astype(bf16)
        else:
            packed = jnp.where(low_lane, change[: lanes // 2], change[lanes // 2 :])
            grown[half, lanes:, :] = packed
            grown_out[half, lanes:, :] = packed.astype(bf16)
    grown_copies = []
    for index in range(2):
        half = 1 - x if index == 0 else x
        grown_copies.append(
            send(
                grown_out.at[half],
                grown_in.at[half],
                grown_send.at[index],
                grown_recv.at[index],
                {"sp": partner, "tp": tp},
            )
        )
    load("wide_proj", wide_proj, proj.at[0])
    load("slim_proj", slim_proj, proj.at[1])
    swaps = []
    for index, (src, dst) in enumerate(
        ((valve_ref, valve), (expand_ref, expand), (contract_ref, contract))
    ):
        load(("expert", index), src, dst.at[core])
        swaps.append(send(src, dst.at[core], swap_send.at[index], swap_recv.at[index], twin))

    loads[0].wait()
    loads[4].wait()

    def turn_queries(block, carry):
        here = pl.ds(pl.multiple_of(block * part, part), part)
        for kind in range(2):
            cosine = tables[2 * kind, here, :]
            sine = tables[2 * kind + 1, here, :]
            for index in range(2):
                piece = staged[4 * kind, here, index * lanes : (index + 1) * lanes]
                turned = jnp.dot(piece, turns[kind], preferred_element_type=f32)
                queries[2 * kind + index, here, :] = (
                    piece.astype(f32) * cosine + turned * sine
                ).astype(bf16)
        return carry

    lax.fori_loop(0, blocks, turn_queries, 0)

    def attend(unit):
        kind, begin = unit_of(unit)
        for block in range(blocks):
            upto = (block + 1) * part
            here = pl.ds(block * part, part)
            query = queries[unit, here, :]
            key = keys[unit, :upto, :]
            value = staged[4 * kind + 2, :upto, begin : begin + lanes]
            spots = iota((part, upto), 1)
            times = iota((part, upto), 0) + block * part
            causal = spots <= times
            apart = (times - spots).astype(f32)
            drop = level[here, 0:1] - surge_line[:, :upto]
            results = []
            for head in range(1 + kind):
                if kind == 0:
                    rate = wide_rate[unit]
                    asked = query
                else:
                    rate = slim_rate[2 * (unit - 2) + head]
                    mine = low_lane if head == 0 else jnp.logical_not(low_lane)
                    asked = jnp.where(mine, query.astype(f32), 0.0).astype(bf16)
                scores = lax.dot_general(
                    asked, key, (((1,), (1,)), ((), ())), preferred_element_type=f32
                )
                gap = apart * rate + drop
                decay = jnp.where(causal, jnp.exp(jnp.where(causal, gap, 0.0)), 0.0)
                results.append(
                    jnp.dot((scores * decay).astype(bf16), value, preferred_element_type=f32)
                )
            result = results[0] if kind == 0 else jnp.where(low_lane, results[0], results[1])
            inner[here, unit * lanes : (unit + 1) * lanes] = result

    attend(0)
    attend(1)

    for copy in tile_copies:
        copy.wait_recv()

    def block_level(place, unit):
        return rates[unit] * length + tiles[place, 1:2, :]

    grown_copies[0].wait_recv()
    mine = grown[x]
    other = grown_in[x].astype(f32)
    first = jnp.where(x == 0, mine, other)
    second = jnp.where(x == 0, other, mine)

    def by_half(wide_values, slim_values):
        return (
            jnp.where(x == 0, wide_values[0], wide_values[1]),
            jnp.where(x == 0, slim_values[0], slim_values[1]),
        )

    def weigh(value, pair):
        return jnp.concatenate([value[:lanes] * pair[0], value[lanes:] * pair[1]], 0)

    odd = [jnp.exp(block_level(2 * group + 1, unit)) for unit in range(4)]
    plane_out[...] = (weigh(first, by_half(odd[:2], odd[2:])) + second).astype(bf16)
    plane_copies = []
    for step in range(1, groups):
        plane_copies.append(
            send(
                plane_out,
                plane_in.at[step],
                plane_send.at[step],
                plane_recv.at[step],
                far[step],
            )
        )

    attend(2)
    attend(3)
    loads[3].wait()
    loads[7].wait()

    def open_gates(block, carry):
        here = pl.ds(pl.multiple_of(block * part, part), part)
        for kind, gain in enumerate((wide_gain, slim_gain)):
            gate = staged[4 * kind + 3, here, :].astype(f32)
            gates[here, 2 * kind * lanes : (2 * kind + 2) * lanes] = gain[...] * jax.nn.silu(gate)
        return carry

    lax.fori_loop(0, blocks, open_gates, 0)
    loads["skip"].wait()
    updated[...] = skip[...].astype(f32)

    carry = jnp.zeros(plane_out.shape, f32)
    reach = [jnp.zeros((1, lanes), f32) for _ in range(4)]
    for step in range(1, groups):
        weight = [jnp.where(group >= step, jnp.exp(reach[unit]), 0.0) for unit in range(4)]
        plane_copies[step - 1].wait_recv()
        carry = carry + weigh(
            plane_in[step].astype(f32), by_half(weight[:2], weight[2:])
        )
        place = lax.rem(group + groups - step, groups)
        for unit in range(4):
            reach[unit] = (
                reach[unit] + block_level(2 * place, unit) + block_level(2 * place + 1, unit)
            )
    carry_out[...] = carry.astype(bf16)
    carry_copy = send(
        carry_out, carry_in, carry_send.at[0], carry_recv.at[0], {"sp": partner, "tp": tp}
    )
    grown_copies[1].wait_recv()
    beside = [
        jnp.where(x == 0, 1.0, jnp.exp(block_level(partner, unit))) for unit in range(4)
    ]
    earlier = jnp.where(x == 0, 0.0, 1.0)
    carry_copy.wait_recv()
    states = [None] * 4
    for half in range(2):
        held = jnp.where(x == half, carry, carry_in[...].astype(f32))
        state = weigh(held, (beside[half], beside[2 + half])) + earlier * grown_in[half].astype(f32)
        states[half] = state[:lanes].astype(bf16)
        slim = state[lanes:]
        states[2 + half] = jnp.concatenate(
            [jnp.where(low_lane, slim, 0.0), jnp.where(low_lane, 0.0, slim)], 0
        ).astype(bf16)

    mixed_copies = []
    for index, owner in enumerate((across, across_twin, twin_tp, tp)):
        begin = pl.multiple_of(owner * part, part)
        here = pl.ds(begin, part)
        moment = (row + begin + 1).astype(f32)
        summed = level[here, :]
        for unit in range(4):
            columns = slice(unit * lanes, (unit + 1) * lanes)
            read = jnp.dot(queries[unit, here, :], states[unit], preferred_element_type=f32)
            factor = jnp.exp(rates[unit] * moment + summed)
            value = inner[here, columns] + factor * read
            square = value * value
            if unit < 2:
                mean = jnp.sum(square, 1, keepdims=True) * (1.0 / BROAD_CHANNEL_DIM)
            else:
                mean = jnp.where(
                    low_lane,
                    jnp.sum(jnp.where(low_lane, square, 0.0), 1, keepdims=True),
                    jnp.sum(jnp.where(low_lane, 0.0, square), 1, keepdims=True),
                ) * (1.0 / THIN_CHANNEL_DIM)
            gated = (value * lax.rsqrt(mean + epsilon) * gates[here, columns]).astype(bf16)
            if index < 3:
                mixed_out[index, :, columns] = gated
            else:
                mixed[tp, :, columns] = gated
        if index < 3:
            mixed_copies.append(
                send(
                    mixed_out.at[index],
                    mixed.at[tp],
                    mixed_send.at[index],
                    mixed_recv.at[index],
                    {"sp": sp, "tp": owner},
                )
            )

    loads["wide_proj"].wait()
    loads["slim_proj"].wait()
    stride = 512
    share_rows = 2 * lanes

    def project(origin):
        above = pl.ds(pl.multiple_of(origin * share_rows, share_rows), share_rows)
        wide = mixed[origin, :, :share_rows]
        slim = mixed[origin, :, share_rows:]

        def one(index, carry):
            column = pl.ds(pl.multiple_of(index * stride, stride), stride)
            updated[:, column] += jnp.dot(
                wide, proj[0, above, column], preferred_element_type=f32
            ) + jnp.dot(slim, proj[1, above, column], preferred_element_type=f32)
            return carry

        lax.fori_loop(0, width // stride, one, 0)

    project(tp)
    mixed_copies[2].wait_recv()
    project(twin_tp)
    mixed_copies[0].wait_recv()
    project(across)
    mixed_copies[1].wait_recv()
    project(across_twin)
    square = jnp.zeros((part, lanes), f32)
    for begin in range(0, width, lanes):
        piece = updated[:, begin : begin + lanes]
        square = square + piece * piece
    scale = lax.rsqrt(jnp.sum(square, 1, keepdims=True) * (1.0 / width) + epsilon)

    def place_rows(index, carry):
        column = pl.ds(pl.multiple_of(index * stride, stride), stride)
        piece = (updated[:, column] * scale * premix_ref[:, column]).astype(bf16)
        spread_rows = lax.dot_general(
            holds[...], piece, (((0,), (0,)), ((), ())), preferred_element_type=f32
        )
        rows[:, :, column] = spread_rows.reshape(groups, cap, stride).astype(bf16)
        return carry

    lax.fori_loop(0, width // stride, place_rows, 0)

    order = [0, 1, 3, 2]
    arriving = {}
    for step in order[1:]:
        arriving[step] = send(
            rows.at[lax.rem(group + step, groups)],
            slots.at[step, 0],
            far_send.at[step],
            far_recv.at[step],
            far[step],
        )
    own = {}

    def spread(step):
        if step > 0:
            arriving[step].wait_recv()
        src = rows.at[group] if step == 0 else slots.at[step, 0]
        own[step] = [
            send(src, slots.at[step, 1], near_send.at[step, 0], near_recv.at[step, 0], near),
            send(src, slots.at[step, 2], near_send.at[step, 1], near_recv.at[step, 1], side),
        ]

    def forward(step):
        own[step][0].wait_recv()
        own[step].append(
            send(
                slots.at[step, 1],
                slots.at[step, 3],
                near_send.at[step, 2],
                near_recv.at[step, 2],
                side,
            )
        )

    spread(0)
    slots[0, 0] = rows[group]
    forward(0)
    spread(order[1])
    near_x = 1 - x + core * (2 * x - 1)
    near_y = y + core * (1 - 2 * y)

    def shares_for(step):
        origin = lax.rem(group + groups - step, groups)
        found = []
        for at_x, at_y in ((x, y), (near_x, near_y), (1 - near_x, 1 - near_y), (1 - x, 1 - y)):
            line = tiles[2 * origin + at_x, 0:1, :]
            pick = iota((cap, lanes), 1) == iota((cap, lanes), 0) + at_y * cap
            found.append(jnp.sum(jnp.where(pick, line, 0.0), 1, keepdims=True))
        return jnp.concatenate(found, 0)

    tile = 256

    def widen(step):
        share = shares_for(step)
        batch = slots[step].reshape(4 * cap, width)

        def one(index, carry):
            half = index // (units // tile)
            begin = pl.multiple_of(lax.rem(index, units // tile) * tile, tile)
            gate = jnp.dot(batch, valve[half, :, pl.ds(begin, tile)], preferred_element_type=f32)
            up = jnp.dot(batch, expand[half, :, pl.ds(begin, tile)], preferred_element_type=f32)
            place = pl.multiple_of(index * tile, tile)
            hidden[:, pl.ds(place, tile)] = (jax.nn.silu(gate) * up * share).astype(bf16)
            return carry

        lax.fori_loop(0, 2 * units // tile, one, 0)

    folding = {}
    joining = {}
    homing = []

    def narrow(step):
        def one(index, carry):
            column = pl.ds(pl.multiple_of(index * stride, stride), stride)
            made = jnp.dot(
                hidden[:, :units], contract[0, :, column], preferred_element_type=f32
            ) + jnp.dot(hidden[:, units:], contract[1, :, column], preferred_element_type=f32)
            kept[step, :, :, column] = made[: 2 * cap].reshape(2, cap, stride)
            leave[step, :, :, column] = made[2 * cap :].reshape(2, cap, stride).astype(bf16)
            return carry

        lax.fori_loop(0, width // stride, one, 0)
        folding[step] = send(
            leave.at[step], landed.at[step], fold_send.at[step, 0], fold_recv.at[step, 0], side
        )

    def join(step):
        folding[step].wait_recv()
        joined[step] = (kept[step, 1] + landed[step, 1].astype(f32)).astype(bf16)
        joining[step] = send(
            joined.at[step], met.at[step], fold_send.at[step, 1], fold_recv.at[step, 1], near
        )
        kept[step, 0] = kept[step, 0] + landed[step, 0].astype(f32)

    def finish_step(step):
        joining[step].wait_recv()
        total = (kept[step, 0] + met[step].astype(f32)).astype(bf16)
        if step == 0:
            returned[group] = total
        else:
            back[step] = total
            homing.append(
                send(
                    back.at[step],
                    returned.at[group],
                    home_send.at[step],
                    home_recv.at[step],
                    far[groups - step],
                )
            )

    for place, step in enumerate(order):
        own[step][1].wait_recv()
        own[step][2].wait_recv()
        if place == 0:
            for index in range(3):
                loads[("expert", index)].wait()
                swaps[index].wait_recv()
        widen(step)
        if place + 1 < groups:
            forward(order[place + 1])
        if place + 2 < groups:
            spread(order[place + 2])
        narrow(step)
        if place >= 1:
            join(order[place - 1])
        if place >= 2:
            finish_step(order[place - 2])
    join(order[-1])
    finish_step(order[-2])
    finish_step(order[-1])
    for copy in homing:
        copy.wait_recv()

    def close(index, carry):
        column = pl.ds(pl.multiple_of(index * stride, stride), stride)
        mixture = jnp.dot(
            holds[...],
            returned[:, :, column].reshape(groups * cap, stride),
            preferred_element_type=f32,
        )
        out_ref[:, column] = (updated[:, column] + mixture).astype(bf16)
        return carry

    lax.fori_loop(0, width // stride, close, 0)
    for copy in sent:
        copy.wait_send()


def rope_table(places):
    found = []
    for size in (BROAD_CHANNEL_DIM, THIN_CHANNEL_DIM):
        half = size // 2
        speed = rope_base ** (-np.arange(half, dtype=np.float64) * 2.0 / size)
        angle = places.astype(np.float64)[:, None] * np.tile(speed, 128 // half)[None, :]
        found += [np.cos(angle), np.sin(angle)]
    return np.stack(found).astype(np.float32)


def whole_layer(*arrays):
    staged = arrays[:8]
    (wide_rate, slim_rate, wide_gain, slim_gain, surge, wide_proj, slim_proj) = arrays[8:15]
    (skip, premix, ids, shares, valve, expand, contract) = arrays[15:]
    kind = skip.dtype
    f32 = jnp.float32
    length = surge.shape[0]
    part, width = skip.shape
    count = lax.axis_size("sp")
    groups = GROUPS
    cap = part * groups // count
    valve, expand, contract = valve[0], expand[0], contract[0]
    units = valve.shape[1]
    lanes = 128
    near_table = jnp.asarray(rope_table(np.arange(length)))
    far_table = jnp.asarray(rope_table(np.arange(count) * length).transpose(1, 0, 2))
    any_spec = pl.BlockSpec(memory_space=pl.ANY)
    smem = pl.BlockSpec(memory_space=pltpu.SMEM)
    dma = pltpu.SemaphoreType.DMA
    packed = lanes + lanes // 2

    def kernel(*refs):
        layer_kernel(refs[:8], *refs[8:])

    return pl.pallas_call(
        kernel,
        out_shape=jax.ShapeDtypeStruct(skip.shape, kind),
        in_specs=[any_spec] * 9
        + [VMEM_SPEC] * 2
        + [smem] * 2
        + [VMEM_SPEC] * 2
        + [any_spec] * 3
        + [VMEM_SPEC] * 3
        + [any_spec] * 3,
        out_specs=VMEM_SPEC,
        scratch_shapes=[
            pltpu.VMEM((8, length, 2 * lanes), kind),
            pltpu.VMEM((4, length, lanes), f32),
            pltpu.VMEM((2,) + wide_proj.shape, kind),
            pltpu.VMEM((part, width), kind),
            pltpu.VMEM((4, length, lanes), kind),
            pltpu.VMEM((4, length, lanes), kind),
            pltpu.VMEM((4, length, lanes), kind),
            pltpu.VMEM((length, lanes), f32),
            pltpu.VMEM((length, 4 * lanes), f32),
            pltpu.VMEM((length, 4 * lanes), f32),
            pltpu.VMEM((2, packed, lanes), f32),
            pltpu.VMEM((2, packed, lanes), kind),
            pltpu.VMEM((2, packed, lanes), kind),
            pltpu.VMEM((count, 8, lanes), f32),
            pltpu.VMEM((count, 8, lanes), f32),
            pltpu.VMEM((packed, lanes), kind),
            pltpu.VMEM((groups, packed, lanes), kind),
            pltpu.VMEM((packed, lanes), kind),
            pltpu.VMEM((packed, lanes), kind),
            pltpu.VMEM((3, part, 4 * lanes), kind),
            pltpu.VMEM((4, part, 4 * lanes), kind),
            pltpu.VMEM((part, width), f32),
            pltpu.VMEM((part, width), kind),
            pltpu.VMEM((part, groups * cap), kind),
            pltpu.VMEM((groups, cap, width), kind),
            pltpu.VMEM((groups, cap, width), kind),
            pltpu.VMEM((groups, 4, cap, width), kind),
            pltpu.VMEM((2,) + valve.shape, kind),
            pltpu.VMEM((2,) + expand.shape, kind),
            pltpu.VMEM((2,) + contract.shape, kind),
            pltpu.VMEM((4 * cap, 2 * units), kind),
            pltpu.VMEM((groups, 2, cap, width), f32),
            pltpu.VMEM((groups, 2, cap, width), kind),
            pltpu.VMEM((groups, 2, cap, width), kind),
            pltpu.VMEM((groups, cap, width), kind),
            pltpu.VMEM((groups, cap, width), kind),
            pltpu.VMEM((groups, cap, width), kind),
            dma((16,)),
            dma((3,)),
            dma((3,)),
            dma((count,)),
            dma((count,)),
            dma((2,)),
            dma((2,)),
            dma((groups,)),
            dma((groups,)),
            dma((1,)),
            dma((1,)),
            dma((3,)),
            dma((3,)),
            dma((groups,)),
            dma((groups,)),
            dma((groups, 3)),
            dma((groups, 3)),
            dma((groups, 2)),
            dma((groups, 2)),
            dma((groups,)),
            dma((groups,)),
        ],
        compiler_params=pltpu.CompilerParams(
            collective_id=3, has_side_effects=True, vmem_limit_bytes=63 * 1024 * 1024
        ),
        name="whole_layer",
    )(
        *staged,
        near_table,
        far_table,
        surge.reshape(1, -1),
        wide_rate,
        slim_rate,
        wide_gain.reshape(1, -1),
        slim_gain.reshape(1, -1),
        wide_proj,
        slim_proj,
        skip,
        premix.reshape(1, -1),
        ids,
        shares,
        valve,
        expand,
        contract,
    )


def rotate(payload_tensor, positions):
    channel_dimension = payload_tensor.shape[-1]
    half = channel_dimension // 2
    freq = rope_base ** (-jnp.arange(half, dtype=jnp.float32) * 2.0 / channel_dimension)
    angle = positions.astype(jnp.float32)[:, None, None] * freq[None, None, :]
    cosine = jnp.cos(angle)
    sine = jnp.sin(angle)
    first = payload_tensor[..., :half]
    second = payload_tensor[..., half:]
    return jnp.concatenate([first * cosine - second * sine, first * sine + second * cosine], -1)


def segment_terms(probe_tensor, lookup_tensor, payload_tensor, surge_forgetting, forgetting_speed):
    length = probe_tensor.shape[0]
    segment_tally = jnp.arange(length, dtype=jnp.float32)
    memory_matrix = (
        forgetting_speed[None, :] * segment_tally[:, None] + jnp.cumsum(surge_forgetting)[:, None]
    )
    causal = (segment_tally[:, None] >= segment_tally[None, :])[None]
    level_t = jnp.transpose(memory_matrix)
    gap = level_t[:, :, None] - level_t[:, None, :]
    decay = jnp.where(causal, jnp.exp(jnp.where(causal, gap, 0.0)), 0.0)
    attention_scores = jnp.einsum(
        "szr,yzr->zsy", probe_tensor, lookup_tensor, preferred_element_type=jnp.float32
    )
    weights = (attention_scores * decay).astype(jnp.bfloat16)
    inner = jnp.einsum("htm,mhe->the", weights, payload_tensor, preferred_element_type=jnp.float32)
    factor = jnp.exp(memory_matrix + forgetting_speed[None, :])
    tail = jnp.exp(memory_matrix[-1:, :] - memory_matrix)
    weighted_output = (lookup_tensor.astype(jnp.float32) * tail[:, :, None]).astype(jnp.bfloat16)
    state_update = jnp.einsum(
        "oup,our->upr", weighted_output, payload_tensor, preferred_element_type=jnp.float32
    )
    total = memory_matrix[-1] + forgetting_speed
    return (inner, factor, state_update, total)


def read_state(probe_tensor, state):
    return jnp.einsum(
        "thd,hde->the", probe_tensor.astype(jnp.float32), state, precision=lax.Precision.HIGHEST
    )


def keeping_multiplier(
    probe_source,
    lookup_tensor,
    payload_tensor,
    forgetting_speed,
    surge_forgetting,
    channel_dimension,
    segment_begin,
):
    length = probe_source.shape[0]
    heads = probe_source.shape[1] // channel_dimension
    places = segment_begin + jnp.arange(length, dtype=jnp.int32)
    spun_probe = rotate(
        probe_source.astype(jnp.float32).reshape(length, heads, channel_dimension), places
    ).astype(jnp.bfloat16)
    spun_lookup = (
        rotate(lookup_tensor.astype(jnp.float32).reshape(length, heads, channel_dimension), places)
        * channel_dimension ** (-0.5)
    ).astype(jnp.bfloat16)
    regrouped_payload = payload_tensor.reshape(length, heads, channel_dimension)
    block = min(512, length)
    count = length // block

    def divider_mark(array):
        return array.reshape((count, block) + array.shape[1:])

    state, level, local, reach = None, None, [], []
    for piece in zip(
        divider_mark(spun_probe),
        divider_mark(spun_lookup),
        divider_mark(regrouped_payload),
        divider_mark(surge_forgetting),
    ):
        inner, factor, state_update, total = segment_terms(*piece, forgetting_speed)
        if state is None:
            state, level = state_update, total
        else:
            inner = inner + factor[:, :, None] * read_state(piece[0], state)
            factor = factor * jnp.exp(level)[None, :]
            state, level = jnp.exp(total)[:, None, None] * state + state_update, level + total
        local.append(inner)
        reach.append(factor)
    return (
        spun_probe,
        jnp.concatenate(local, 0),
        jnp.concatenate(reach, 0),
        level,
        state,
    )


def finish(sublayer_final, emission_valve, scaling_coefficients):
    length, heads, channel_dimension = sublayer_final.shape
    normed = sublayer_final * lax.rsqrt(
        jnp.mean(sublayer_final * sublayer_final, -1, keepdims=True) + epsilon
    )
    gated = (
        normed.reshape(length, heads * channel_dimension)
        * scaling_coefficients[None, :]
        * jax.nn.silu(emission_valve.astype(jnp.float32))
    )
    return gated.astype(jnp.bfloat16)


def carried(states, levels):
    place = lax.axis_index("sp")
    count = states.shape[0]
    index = jnp.arange(count, dtype=jnp.int32)
    between = (index[None, :] > index[:, None]) & (index[None, :] < place)
    reach = jnp.sum(jnp.where(between[:, :, None], levels[None, :, :], 0.0), 1)
    weight = jnp.where((index < place)[:, None], jnp.exp(reach), 0.0)
    return jnp.sum(weight[:, :, None, None] * states.astype(jnp.float32), 0)


def slot_positions(chosen, experts, cap):
    listed = chosen.reshape(-1)
    matches = (listed[:, None] == jnp.arange(experts, dtype=jnp.int32)[None, :]).astype(jnp.int32)
    before = jnp.cumsum(matches, 0) - matches
    order = jnp.sum(before * matches, 1)
    return (listed * cap + order).reshape(chosen.shape)


def fill_slots(rows_in, chosen, experts, cap):
    count = rows_in.shape[0]
    places = slot_positions(chosen, experts, cap).reshape(-1)
    owners = jnp.repeat(jnp.arange(count, dtype=jnp.int32), 2)
    source = jnp.full((experts * cap,), count, jnp.int32).at[places].set(owners)
    padded = jnp.concatenate([rows_in, jnp.zeros((1, rows_in.shape[1]), rows_in.dtype)], 0)
    return padded[source].reshape(experts, cap, rows_in.shape[1])


def served(wide, slim, skip, valve):
    return (
        lax.axis_size("sp") * valve.shape[0] == 2 * GROUPS
        and lax.axis_size("tp") == 4
        and wide.shape[1] == slim.shape[1] == 2 * BROAD_CHANNEL_DIM
        and skip.shape[0] == 128
        and wide.shape[0] == 4 * skip.shape[0]
    )


def on_device(
    broad_probe_tensor,
    broad_lookup_tensor,
    broad_payload_tensor,
    broad_emission_valve,
    slim_probe_tensor,
    slim_lookup_tensor,
    slim_payload_tensor,
    slim_emission_valve,
    broad_forgetting_speed,
    slim_forgetting_speed,
    broad_channel_scaling,
    slim_channel_scaling,
    surge_forgetting,
    broad_emission_proj,
    slim_emission_proj,
    skip_stream,
    premix_scaling_coeffs,
    routed_specialist_ids,
    routed_specialist_shares,
    specialist_valve_proj,
    specialist_expand_proj,
    specialist_contract_proj,
):
    length = broad_probe_tensor.shape[0]
    segment_begin = lax.axis_index("sp") * length
    if served(broad_probe_tensor, slim_probe_tensor, skip_stream, specialist_valve_proj):
        return whole_layer(
            broad_probe_tensor,
            broad_lookup_tensor,
            broad_payload_tensor,
            broad_emission_valve,
            slim_probe_tensor,
            slim_lookup_tensor,
            slim_payload_tensor,
            slim_emission_valve,
            broad_forgetting_speed,
            slim_forgetting_speed,
            broad_channel_scaling,
            slim_channel_scaling,
            surge_forgetting,
            broad_emission_proj,
            slim_emission_proj,
            skip_stream,
            premix_scaling_coeffs,
            routed_specialist_ids,
            routed_specialist_shares,
            specialist_valve_proj,
            specialist_expand_proj,
            specialist_contract_proj,
        )
    valve_all = lax.all_gather(specialist_valve_proj[0], "tp")
    expand_all = lax.all_gather(specialist_expand_proj[0], "tp")
    contract_all = lax.all_gather(specialist_contract_proj[0], "tp")
    wide_result = keeping_multiplier(
        broad_probe_tensor,
        broad_lookup_tensor,
        broad_payload_tensor,
        broad_forgetting_speed,
        surge_forgetting,
        BROAD_CHANNEL_DIM,
        segment_begin,
    )
    narrow_result = keeping_multiplier(
        slim_probe_tensor,
        slim_lookup_tensor,
        slim_payload_tensor,
        slim_forgetting_speed,
        surge_forgetting,
        THIN_CHANNEL_DIM,
        segment_begin,
    )
    rows = skip_stream.shape[0]
    width = skip_stream.shape[1]
    experts = lax.axis_size("sp") * specialist_valve_proj.shape[0]
    cap = rows * GROUPS // experts
    pair = experts // GROUPS
    own_ids = lax.dynamic_slice_in_dim(routed_specialist_ids, lax.axis_index("tp") * rows, rows, 0)
    own_weights = lax.dynamic_slice_in_dim(
        routed_specialist_shares, lax.axis_index("tp") * rows, rows, 0
    )
    levels = jnp.concatenate([wide_result[3], narrow_result[3]])
    tile = levels
    tile_size = -(-tile.shape[0] // 1024) * 1024
    tile = jnp.pad(tile, (0, tile_size - tile.shape[0])).reshape(-1, 128)
    packed = jnp.concatenate(
        [wide_result[4].reshape(-1, 128), narrow_result[4].reshape(-1, 128)], 0
    ).astype(jnp.bfloat16)
    states, tiles = exchange(packed, tile)
    count = states.shape[0]
    tiles = tiles.reshape(count, -1)
    wide_heads = wide_result[3].shape[0]
    both_heads = levels.shape[0]
    cut = wide_result[4].size // 128
    incoming_wide = carried(
        states[:, :cut].reshape((count,) + wide_result[4].shape), tiles[:, :wide_heads]
    )
    incoming_narrow = carried(
        states[:, cut:].reshape((count,) + narrow_result[4].shape),
        tiles[:, wide_heads:both_heads],
    )
    mixed_wide = finish(
        wide_result[1] + wide_result[2][:, :, None] * read_state(wide_result[0], incoming_wide),
        broad_emission_valve,
        broad_channel_scaling,
    )
    mixed_narrow = finish(
        narrow_result[1] + narrow_result[2][:, :, None] * read_state(narrow_result[0], incoming_narrow),
        slim_emission_valve,
        slim_channel_scaling,
    )
    rows_wide, rows_narrow = (
        lax.all_to_all(mixed_wide, "tp", split_axis=0, concat_axis=1, tiled=True),
        lax.all_to_all(mixed_narrow, "tp", split_axis=0, concat_axis=1, tiled=True),
    )
    projected = jnp.dot(rows_wide, broad_emission_proj, preferred_element_type=jnp.float32)
    projected = projected + jnp.dot(
        rows_narrow, slim_emission_proj, preferred_element_type=jnp.float32
    )
    updated = skip_stream.astype(jnp.float32) + projected
    scale = lax.rsqrt(jnp.mean(updated * updated, -1, keepdims=True) + epsilon)
    normed = (updated * scale * premix_scaling_coeffs[None, :]).astype(jnp.bfloat16)
    own_places = slot_positions(own_ids, experts, cap)
    slots = lax.all_to_all(
        fill_slots(normed, own_ids, experts, cap), "sp", split_axis=0, concat_axis=0, tiled=True
    ).reshape(-1, width)
    expert_out = None
    for part in range(lax.axis_size("tp")):
        emission_valve = jnp.dot(slots, valve_all[part], preferred_element_type=jnp.float32)
        up = jnp.dot(slots, expand_all[part], preferred_element_type=jnp.float32)
        hidden = (jax.nn.silu(emission_valve) * up).astype(jnp.bfloat16)
        term = jnp.dot(hidden, contract_all[part], preferred_element_type=jnp.float32)
        expert_out = term if expert_out is None else expert_out + term
    returned = lax.all_to_all(
        expert_out.astype(jnp.bfloat16).reshape(experts, cap, width),
        "sp",
        split_axis=0,
        concat_axis=0,
        tiled=True,
    )
    picked = returned.reshape(experts * cap, width)[own_places]
    mixture = jnp.sum(own_weights[:, :, None] * picked.astype(jnp.float32), 1)
    return (updated + mixture).astype(jnp.bfloat16)


def solution(mesh):
    return jax.shard_map(
        on_device,
        mesh=mesh,
        in_specs=(
            P("sp", "tp"),
            P("sp", "tp"),
            P("sp", "tp"),
            P("sp", "tp"),
            P("sp", "tp"),
            P("sp", "tp"),
            P("sp", "tp"),
            P("sp", "tp"),
            P("tp"),
            P("tp"),
            P("tp"),
            P("tp"),
            P("sp"),
            P(),
            P(),
            P(("sp", "tp"), None),
            P(),
            P("sp", None),
            P("sp", None),
            P("sp", None, "tp"),
            P("sp", None, "tp"),
            P("sp", "tp", None),
        ),
        out_specs=P(("sp", "tp"), None),
        check_vma=False,
    )
```

```python
import jax
import jax.numpy as jnp
import numpy as np
from jax import lax
from jax.experimental import pallas as pl
from jax.experimental.pallas import tpu as pltpu
from jax.sharding import PartitionSpec as P

MESH = pl.DeviceIdType.MESH
VMEM_SPEC = pl.BlockSpec(memory_space=pltpu.VMEM)

BROAD_CHANNEL_DIM = 128
THIN_CHANNEL_DIM = 64
GROUPS = 4


rope_base = 10000.0
epsilon = 1e-06


def exchange_kernel(state_ref, tile_ref, states_ref, tiles_ref, send_sem, recv_sem):
    me = lax.axis_index("sp")
    count = states_ref.shape[0]
    barrier = pltpu.get_barrier_semaphore()
    for step in range(1, count):
        pl.semaphore_signal(
            barrier, inc=1, device_id={"sp": lax.rem(me + step, count)}, device_id_type=MESH
        )
    pl.semaphore_wait(barrier, count - 1)
    copies = []
    for step in range(1, count):
        for kind, (src, dst) in enumerate(((state_ref, states_ref), (tile_ref, tiles_ref))):
            copy = pltpu.make_async_remote_copy(
                src_ref=src,
                dst_ref=dst.at[me],
                send_sem=send_sem.at[kind, step],
                recv_sem=recv_sem.at[kind, step],
                device_id={"sp": lax.rem(me + step, count)},
                device_id_type=MESH,
            )
            copy.start()
            copies.append(copy)
    states_ref[me] = state_ref[...]
    tiles_ref[me] = tile_ref[...]
    for copy in copies:
        copy.wait()


def exchange(state, tile):
    count = lax.axis_size("sp")
    return pl.pallas_call(
        exchange_kernel,
        out_shape=(
            jax.ShapeDtypeStruct((count,) + state.shape, state.dtype),
            jax.ShapeDtypeStruct((count,) + tile.shape, tile.dtype),
        ),
        in_specs=[VMEM_SPEC] * 2,
        out_specs=(VMEM_SPEC, VMEM_SPEC),
        scratch_shapes=[
            pltpu.SemaphoreType.DMA((2, count)),
            pltpu.SemaphoreType.DMA((2, count)),
        ],
        compiler_params=pltpu.CompilerParams(collective_id=0, has_side_effects=True),
        name="state_exchange",
    )(state, tile)


def places_of(groups):
    sp = lax.axis_index("sp")
    tp = lax.axis_index("tp")
    core = lax.rem(tp, 2)
    x = lax.rem(sp, 2)
    y = tp // 2
    across_sp = sp + 1 - 2 * x
    across_tp = tp + 2 - 4 * y
    near = {"sp": across_sp + core * (sp - across_sp), "tp": tp + core * (across_tp - tp)}
    side = {"sp": sp + core * (across_sp - sp), "tp": across_tp + core * (tp - across_tp)}
    twin = {"sp": sp, "tp": tp + 1 - 2 * core}
    group = sp // 2
    far = [{"sp": lax.rem(group + step, groups) * 2 + x, "tp": tp} for step in range(groups)]
    return group, x, y, core, near, side, twin, far


def layer_kernel(
    inputs,
    tables_ref,
    turn_ref,
    surge_ref,
    wide_rate,
    slim_rate,
    wide_gain,
    slim_gain,
    wide_proj,
    slim_proj,
    skip_ref,
    premix_ref,
    ids_ref,
    share_ref,
    valve_ref,
    expand_ref,
    contract_ref,
    out_ref,
    staged,
    tables,
    proj,
    skip,
    queries,
    keys,
    faded,
    level,
    inner,
    gates,
    grown,
    grown_out,
    grown_in,
    tile_out,
    tiles,
    plane_out,
    plane_in,
    carry_out,
    carry_in,
    mixed_out,
    mixed,
    updated,
    normed,
    holds,
    rows,
    returned,
    slots,
    valve,
    expand,
    contract,
    hidden,
    kept,
    leave,
    landed,
    joined,
    met,
    back,
    load_sem,
    swap_send,
    swap_recv,
    tile_send,
    tile_recv,
    grown_send,
    grown_recv,
    plane_send,
    plane_recv,
    carry_send,
    carry_recv,
    mixed_send,
    mixed_recv,
    far_send,
    far_recv,
    near_send,
    near_recv,
    fold_send,
    fold_recv,
    home_send,
    home_recv,
):
    f32 = jnp.float32
    bf16 = jnp.bfloat16
    groups, cap, width = rows.shape
    units = valve_ref.shape[1]
    length = staged.shape[1]
    part = skip.shape[0]
    lanes = 128
    blocks = length // part
    count = tiles.shape[0]
    sp = lax.axis_index("sp")
    tp = lax.axis_index("tp")
    group, x, y, core, near, side, twin, far = places_of(groups)
    partner = sp + 1 - 2 * x
    across = tp + 2 - 4 * y
    twin_tp = tp + 1 - 2 * core
    across_twin = twin_tp + 2 - 4 * y

    loads = {}

    def load(name, src, dst):
        copy = pltpu.make_async_copy(src, dst, load_sem.at[len(loads)])
        copy.start()
        loads[name] = copy

    for index in (1, 5):
        load(index, inputs[index], staged.at[index])
    load("tables", tables_ref, tables)
    for index in (2, 6, 0, 4, 3, 7):
        load(index, inputs[index], staged.at[index])
    load("skip", skip_ref, skip)

    barrier = pltpu.get_barrier_semaphore()
    friends = [{"sp": lax.rem(sp + step, count), "tp": tp} for step in range(1, count)]
    friends += [{"sp": sp, "tp": other} for other in (across, twin_tp, across_twin)]
    for friend in friends:
        pl.semaphore_signal(barrier, inc=1, device_id=friend, device_id_type=MESH)
    pl.semaphore_wait(barrier, len(friends))
    sent = []

    def send(src, dst, send_sem, recv_sem, device):
        copy = pltpu.make_async_remote_copy(
            src_ref=src,
            dst_ref=dst,
            send_sem=send_sem,
            recv_sem=recv_sem,
            device_id=device,
            device_id_type=MESH,
        )
        copy.start()
        sent.append(copy)
        return copy

    def iota(shape, axis):
        return lax.broadcasted_iota(jnp.int32, shape, axis)

    lane = iota((part, lanes), 1)
    row = iota((part, lanes), 0)
    eye = lane == row
    low_lane = iota((1, lanes), 1) < lanes // 2

    surge = surge_ref[...]
    wide_lane = iota((part, length), 1)
    wide_row = iota((part, length), 0)
    lines = []
    for block in range(blocks):
        column = jnp.sum(
            jnp.where(wide_lane <= wide_row + block * part, surge, 0.0), 1, keepdims=True
        )
        level[pl.ds(block * part, part), :] = jnp.broadcast_to(column, (part, lanes))
        lines.append(jnp.sum(jnp.where(eye, column, 0.0), 0, keepdims=True))
    surge_line = jnp.concatenate(lines, 1)
    surge_total = jnp.broadcast_to(jnp.sum(surge, 1, keepdims=True), (1, lanes))

    rates = [
        jnp.full((1, lanes), wide_rate[0], f32),
        jnp.full((1, lanes), wide_rate[1], f32),
        jnp.where(low_lane, slim_rate[0], slim_rate[1]),
        jnp.where(low_lane, slim_rate[2], slim_rate[3]),
    ]

    def route(block):
        begin = pl.multiple_of(block * part, part)
        ids = ids_ref[0:1, pl.ds(begin, part)]
        weights = share_ref[:, pl.ds(begin, part)]
        first = jnp.sum(jnp.where(eye, ids, 0), 1, keepdims=True)
        weights = [
            jnp.sum(jnp.where(eye, weights[choice : choice + 1], 0.0), 1, keepdims=True)
            for choice in range(2)
        ]
        chosen = lax.shift_right_logical(first, 1)
        named = chosen == lane
        rank = jnp.dot(
            jnp.where(row >= lane, 1.0, 0.0).astype(bf16),
            jnp.where(named, 1.0, 0.0).astype(bf16),
            preferred_element_type=f32,
        )
        order_in = jnp.sum(jnp.where(named, rank, 0.0), 1, keepdims=True).astype(jnp.int32) - 1
        even = first - 2 * chosen == 0
        shares = [
            jnp.where(even, weights[0], weights[1]),
            jnp.where(even, weights[1], weights[0]),
        ]
        return chosen, order_in, shares

    chosen, order_in, _ = route(tp)
    holds[...] = jnp.where(
        chosen * cap + order_in == iota((part, groups * cap), 1), 1.0, 0.0
    ).astype(bf16)
    share_lines = [0.0, 0.0]
    for block_y in range(2):
        chosen, order_in, shares = route(2 * block_y + core)
        here = chosen * (2 * cap) + block_y * cap + order_in == iota((part, 2 * groups * cap), 1)
        for member in range(2):
            share_lines[member] = share_lines[member] + jnp.sum(
                jnp.where(here, shares[member], 0.0), 0, keepdims=True
            )
    top = iota((8, lanes), 0) == 0
    for target in range(count):
        line = share_lines[target % 2][:, (target // 2) * lanes : (target // 2 + 1) * lanes]
        tile_out[target] = jnp.where(top, line, surge_total)
    tile_copies = []
    for step in range(1, count):
        other = lax.rem(sp + step, count)
        tile_copies.append(
            send(
                tile_out.at[other],
                tiles.at[sp],
                tile_send.at[step],
                tile_recv.at[step],
                {"sp": other, "tp": tp},
            )
        )
    tiles[sp] = tile_out[sp]

    def turner(size):
        half = size // 2
        low = lax.rem(lane, size) < half
        match = row == jnp.where(low, lane + half, lane - half)
        return jnp.where(match, jnp.where(low, -1.0, 1.0), 0.0).astype(bf16)

    turns = [turner(BROAD_CHANNEL_DIM), turner(THIN_CHANNEL_DIM)]
    scales = [BROAD_CHANNEL_DIM ** (-0.5), THIN_CHANNEL_DIM ** (-0.5)]
    turn = turn_ref[sp]

    def unit_of(index):
        return index // 2, (index % 2) * lanes

    loads["tables"].wait()
    loads[1].wait()
    loads[5].wait()
    last = [rates[unit] * (length - 1) + surge_total for unit in range(4)]

    def turn_keys(block, carry):
        here = pl.ds(pl.multiple_of(block * part, part), part)
        moment = (row + block * part).astype(f32)
        summed = level[here, :]
        for kind in range(2):
            cosine_near = tables[2 * kind, here, :]
            sine_near = tables[2 * kind + 1, here, :]
            cosine_far = turn[2 * kind : 2 * kind + 1]
            sine_far = turn[2 * kind + 1 : 2 * kind + 2]
            cosine = cosine_near * cosine_far - sine_near * sine_far
            sine = sine_near * cosine_far + cosine_near * sine_far
            tables[2 * kind, here, :] = cosine
            tables[2 * kind + 1, here, :] = sine
            for index in range(2):
                unit = 2 * kind + index
                piece = staged[4 * kind + 1, here, index * lanes : (index + 1) * lanes]
                turned = jnp.dot(piece, turns[kind], preferred_element_type=f32)
                key = (
                    (piece.astype(f32) * cosine + turned * sine) * scales[kind]
                ).astype(bf16)
                keys[unit, here, :] = key
                tail = jnp.exp(last[unit] - (rates[unit] * moment + summed))
                faded[unit, here, :] = (key.astype(f32) * tail).astype(bf16)
        return carry

    lax.fori_loop(0, blocks, turn_keys, 0)
    loads[2].wait()
    loads[6].wait()
    for unit in range(4):
        kind, begin = unit_of(unit)
        change = lax.dot_general(
            faded[unit],
            staged[4 * kind + 2, :, begin : begin + lanes],
            (((0,), (0,)), ((), ())),
            preferred_element_type=f32,
        )
        half = unit % 2
        if kind == 0:
            grown[half, :lanes, :] = change
            grown_out[half, :lanes, :] = change.astype(bf16)
        else:
            packed = jnp.where(low_lane, change[: lanes // 2], change[lanes // 2 :])
            grown[half, lanes:, :] = packed
            grown_out[half, lanes:, :] = packed.astype(bf16)
    grown_copies = []
    for index in range(2):
        half = 1 - x if index == 0 else x
        grown_copies.append(
            send(
                grown_out.at[half],
                grown_in.at[half],
                grown_send.at[index],
                grown_recv.at[index],
                {"sp": partner, "tp": tp},
            )
        )
    load("wide_proj", wide_proj, proj.at[0])
    load("slim_proj", slim_proj, proj.at[1])
    swaps = []
    for index, (src, dst) in enumerate(
        ((valve_ref, valve), (expand_ref, expand), (contract_ref, contract))
    ):
        load(("expert", index), src, dst.at[core])
        swaps.append(send(src, dst.at[core], swap_send.at[index], swap_recv.at[index], twin))

    loads[0].wait()
    loads[4].wait()

    def turn_queries(block, carry):
        here = pl.ds(pl.multiple_of(block * part, part), part)
        for kind in range(2):
            cosine = tables[2 * kind, here, :]
            sine = tables[2 * kind + 1, here, :]
            for index in range(2):
                piece = staged[4 * kind, here, index * lanes : (index + 1) * lanes]
                turned = jnp.dot(piece, turns[kind], preferred_element_type=f32)
                queries[2 * kind + index, here, :] = (
                    piece.astype(f32) * cosine + turned * sine
                ).astype(bf16)
        return carry

    lax.fori_loop(0, blocks, turn_queries, 0)

    def attend(unit):
        kind, begin = unit_of(unit)
        for block in range(blocks):
            upto = (block + 1) * part
            here = pl.ds(block * part, part)
            query = queries[unit, here, :]
            key = keys[unit, :upto, :]
            value = staged[4 * kind + 2, :upto, begin : begin + lanes]
            spots = iota((part, upto), 1)
            times = iota((part, upto), 0) + block * part
            causal = spots <= times
            apart = (times - spots).astype(f32)
            drop = level[here, 0:1] - surge_line[:, :upto]
            results = []
            for head in range(1 + kind):
                if kind == 0:
                    rate = wide_rate[unit]
                    asked = query
                else:
                    rate = slim_rate[2 * (unit - 2) + head]
                    mine = low_lane if head == 0 else jnp.logical_not(low_lane)
                    asked = jnp.where(mine, query.astype(f32), 0.0).astype(bf16)
                scores = lax.dot_general(
                    asked, key, (((1,), (1,)), ((), ())), preferred_element_type=f32
                )
                gap = apart * rate + drop
                decay = jnp.where(causal, jnp.exp(jnp.where(causal, gap, 0.0)), 0.0)
                results.append(
                    jnp.dot((scores * decay).astype(bf16), value, preferred_element_type=f32)
                )
            result = results[0] if kind == 0 else jnp.where(low_lane, results[0], results[1])
            inner[here, unit * lanes : (unit + 1) * lanes] = result

    attend(0)
    attend(1)

    for copy in tile_copies:
        copy.wait_recv()

    def block_level(place, unit):
        return rates[unit] * length + tiles[place, 1:2, :]

    grown_copies[0].wait_recv()
    mine = grown[x]
    other = grown_in[x].astype(f32)
    first = jnp.where(x == 0, mine, other)
    second = jnp.where(x == 0, other, mine)

    def by_half(wide_values, slim_values):
        return (
            jnp.where(x == 0, wide_values[0], wide_values[1]),
            jnp.where(x == 0, slim_values[0], slim_values[1]),
        )

    def weigh(value, pair):
        return jnp.concatenate([value[:lanes] * pair[0], value[lanes:] * pair[1]], 0)

    odd = [jnp.exp(block_level(2 * group + 1, unit)) for unit in range(4)]
    plane_out[...] = (weigh(first, by_half(odd[:2], odd[2:])) + second).astype(bf16)
    plane_copies = []
    for step in range(1, groups):
        plane_copies.append(
            send(
                plane_out,
                plane_in.at[step],
                plane_send.at[step],
                plane_recv.at[step],
                far[step],
            )
        )

    attend(2)
    attend(3)
    loads[3].wait()
    loads[7].wait()

    def open_gates(block, carry):
        here = pl.ds(pl.multiple_of(block * part, part), part)
        for kind, gain in enumerate((wide_gain, slim_gain)):
            gate = staged[4 * kind + 3, here, :].astype(f32)
            gates[here, 2 * kind * lanes : (2 * kind + 2) * lanes] = gain[...] * jax.nn.silu(gate)
        return carry

    lax.fori_loop(0, blocks, open_gates, 0)
    loads["skip"].wait()
    updated[...] = skip[...].astype(f32)

    carry = jnp.zeros(plane_out.shape, f32)
    reach = [jnp.zeros((1, lanes), f32) for _ in range(4)]
    for step in range(1, groups):
        weight = [jnp.where(group >= step, jnp.exp(reach[unit]), 0.0) for unit in range(4)]
        plane_copies[step - 1].wait_recv()
        carry = carry + weigh(
            plane_in[step].astype(f32), by_half(weight[:2], weight[2:])
        )
        place = lax.rem(group + groups - step, groups)
        for unit in range(4):
            reach[unit] = (
                reach[unit] + block_level(2 * place, unit) + block_level(2 * place + 1, unit)
            )
    carry_out[...] = carry.astype(bf16)
    carry_copy = send(
        carry_out, carry_in, carry_send.at[0], carry_recv.at[0], {"sp": partner, "tp": tp}
    )
    grown_copies[1].wait_recv()
    beside = [
        jnp.where(x == 0, 1.0, jnp.exp(block_level(partner, unit))) for unit in range(4)
    ]
    earlier = jnp.where(x == 0, 0.0, 1.0)
    carry_copy.wait_recv()
    states = [None] * 4
    for half in range(2):
        held = jnp.where(x == half, carry, carry_in[...].astype(f32))
        state = weigh(held, (beside[half], beside[2 + half])) + earlier * grown_in[half].astype(f32)
        states[half] = state[:lanes].astype(bf16)
        slim = state[lanes:]
        states[2 + half] = jnp.concatenate(
            [jnp.where(low_lane, slim, 0.0), jnp.where(low_lane, 0.0, slim)], 0
        ).astype(bf16)

    mixed_copies = []
    for index, owner in enumerate((across, across_twin, twin_tp, tp)):
        begin = pl.multiple_of(owner * part, part)
        here = pl.ds(begin, part)
        moment = (row + begin + 1).astype(f32)
        summed = level[here, :]
        for unit in range(4):
            columns = slice(unit * lanes, (unit + 1) * lanes)
            read = jnp.dot(queries[unit, here, :], states[unit], preferred_element_type=f32)
            factor = jnp.exp(rates[unit] * moment + summed)
            value = inner[here, columns] + factor * read
            square = value * value
            if unit < 2:
                mean = jnp.sum(square, 1, keepdims=True) * (1.0 / BROAD_CHANNEL_DIM)
            else:
                mean = jnp.where(
                    low_lane,
                    jnp.sum(jnp.where(low_lane, square, 0.0), 1, keepdims=True),
                    jnp.sum(jnp.where(low_lane, 0.0, square), 1, keepdims=True),
                ) * (1.0 / THIN_CHANNEL_DIM)
            gated = (value * lax.rsqrt(mean + epsilon) * gates[here, columns]).astype(bf16)
            if index < 3:
                mixed_out[index, :, columns] = gated
            else:
                mixed[tp, :, columns] = gated
        if index < 3:
            mixed_copies.append(
                send(
                    mixed_out.at[index],
                    mixed.at[tp],
                    mixed_send.at[index],
                    mixed_recv.at[index],
                    {"sp": sp, "tp": owner},
                )
            )

    loads["wide_proj"].wait()
    loads["slim_proj"].wait()
    stride = 512
    share_rows = 2 * lanes

    def project(origin):
        above = pl.ds(pl.multiple_of(origin * share_rows, share_rows), share_rows)
        wide = mixed[origin, :, :share_rows]
        slim = mixed[origin, :, share_rows:]

        def one(index, carry):
            column = pl.ds(pl.multiple_of(index * stride, stride), stride)
            updated[:, column] += jnp.dot(
                wide, proj[0, above, column], preferred_element_type=f32
            ) + jnp.dot(slim, proj[1, above, column], preferred_element_type=f32)
            return carry

        lax.fori_loop(0, width // stride, one, 0)

    project(tp)
    mixed_copies[2].wait_recv()
    project(twin_tp)
    mixed_copies[0].wait_recv()
    project(across)
    mixed_copies[1].wait_recv()
    project(across_twin)
    square = jnp.zeros((part, lanes), f32)
    for begin in range(0, width, lanes):
        piece = updated[:, begin : begin + lanes]
        square = square + piece * piece
    scale = lax.rsqrt(jnp.sum(square, 1, keepdims=True) * (1.0 / width) + epsilon)

    def place_rows(index, carry):
        column = pl.ds(pl.multiple_of(index * stride, stride), stride)
        piece = (updated[:, column] * scale * premix_ref[:, column]).astype(bf16)
        spread_rows = lax.dot_general(
            holds[...], piece, (((0,), (0,)), ((), ())), preferred_element_type=f32
        )
        rows[:, :, column] = spread_rows.reshape(groups, cap, stride).astype(bf16)
        return carry

    lax.fori_loop(0, width // stride, place_rows, 0)

    order = [1, 3, 2, 0]
    piece_rows = cap // 2

    def piece(portion):
        return pl.ds(portion * piece_rows, piece_rows)

    arriving = {}
    for step in order[:3]:
        for portion in range(2):
            arriving[step, portion] = send(
                rows.at[lax.rem(group + step, groups), piece(portion)],
                slots.at[step, 0, piece(portion)],
                far_send.at[step, portion],
                far_recv.at[step, portion],
                far[step],
            )
    own = {}

    def spread(step):
        for portion in range(2):
            here = piece(portion)
            if step > 0:
                arriving[step, portion].wait_recv()
            src = rows.at[group, here] if step == 0 else slots.at[step, 0, here]
            for place, device in ((1, near), (2, side)):
                own[step, place, portion] = send(
                    src,
                    slots.at[step, place, here],
                    near_send.at[step, 2 * place - 2 + portion],
                    near_recv.at[step, 2 * place - 2 + portion],
                    device,
                )

    def forward(step):
        for portion in range(2):
            here = piece(portion)
            own[step, 1, portion].wait_recv()
            own[step, 3, portion] = send(
                slots.at[step, 1, here],
                slots.at[step, 3, here],
                near_send.at[step, 4 + portion],
                near_recv.at[step, 4 + portion],
                side,
            )

    spread(0)
    slots[0, 0] = rows[group]
    forward(0)
    spread(order[0])
    forward(order[0])
    spread(order[1])
    near_x = 1 - x + core * (2 * x - 1)
    near_y = y + core * (1 - 2 * y)

    def shares_for(step):
        origin = lax.rem(group + groups - step, groups)
        found = []
        for at_x, at_y in ((x, y), (near_x, near_y), (1 - near_x, 1 - near_y), (1 - x, 1 - y)):
            line = tiles[2 * origin + at_x, 0:1, :]
            pick = iota((cap, lanes), 1) == iota((cap, lanes), 0) + at_y * cap
            found.append(jnp.sum(jnp.where(pick, line, 0.0), 1, keepdims=True))
        return jnp.concatenate(found, 0)

    tile = 256

    def widen(step, portion):
        share = shares_for(step)
        batch = slots[step].reshape(4 * cap, width)

        def one(index, carry):
            half = index // (units // tile)
            begin = pl.multiple_of(lax.rem(index, units // tile) * tile, tile)
            gate = jnp.dot(batch, valve[half, :, pl.ds(begin, tile)], preferred_element_type=f32)
            up = jnp.dot(batch, expand[half, :, pl.ds(begin, tile)], preferred_element_type=f32)
            place = pl.multiple_of(index * tile, tile)
            hidden[:, pl.ds(place, tile)] = (jax.nn.silu(gate) * up * share).astype(bf16)
            return carry

        count_tiles = 2 * units // tile // 2
        lax.fori_loop(portion * count_tiles, (portion + 1) * count_tiles, one, 0)

    folding = {}
    joining = {}
    homing = []
    span = width // 2

    def columns_of(portion):
        return pl.ds(portion * span, span)

    def narrow(step):
        for portion in range(2):

            def one(index, carry):
                column = pl.ds(pl.multiple_of(index * stride, stride), stride)
                made = jnp.dot(
                    hidden[:, :units], contract[0, :, column], preferred_element_type=f32
                ) + jnp.dot(hidden[:, units:], contract[1, :, column], preferred_element_type=f32)
                kept[step, :, :, column] = made[: 2 * cap].reshape(2, cap, stride)
                leave[step, :, :, column] = made[2 * cap :].reshape(2, cap, stride).astype(bf16)
                return carry

            count_tiles = span // stride
            lax.fori_loop(portion * count_tiles, (portion + 1) * count_tiles, one, 0)
            column = columns_of(portion)
            folding[step, portion] = send(
                leave.at[step, :, :, column],
                landed.at[step, :, :, column],
                fold_send.at[step, portion],
                fold_recv.at[step, portion],
                side,
            )

    def join(step):
        for portion in range(2):
            column = columns_of(portion)
            folding[step, portion].wait_recv()
            joined[step, :, column] = (
                kept[step, 1, :, column] + landed[step, 1, :, column].astype(f32)
            ).astype(bf16)
            joining[step, portion] = send(
                joined.at[step, :, column],
                met.at[step, :, column],
                fold_send.at[step, 2 + portion],
                fold_recv.at[step, 2 + portion],
                near,
            )

    def finish_step(step):
        for portion in range(2):
            column = columns_of(portion)
            joining[step, portion].wait_recv()
            total = (
                kept[step, 0, :, column]
                + landed[step, 0, :, column].astype(f32)
                + met[step, :, column].astype(f32)
            ).astype(bf16)
            if step == 0:
                returned[group, :, column] = total
            else:
                back[step, :, column] = total
                homing.append(
                    send(
                        back.at[step, :, column],
                        returned.at[group, :, column],
                        home_send.at[step, portion],
                        home_recv.at[step, portion],
                        far[groups - step],
                    )
                )

    def gathered(step):
        for portion in range(2):
            own[step, 2, portion].wait_recv()
            own[step, 3, portion].wait_recv()

    for index in range(3):
        loads[("expert", index)].wait()
        swaps[index].wait_recv()
    gathered(order[0])
    widen(order[0], 0)
    spread(order[2])
    widen(order[0], 1)
    forward(order[1])
    narrow(order[0])
    gathered(order[1])
    widen(order[1], 0)
    forward(order[2])
    widen(order[1], 1)
    narrow(order[1])
    join(order[0])
    gathered(order[2])
    widen(order[2], 0)
    finish_step(order[0])
    widen(order[2], 1)
    narrow(order[2])
    join(order[1])
    gathered(order[3])
    widen(order[3], 0)
    finish_step(order[1])
    widen(order[3], 1)
    narrow(order[3])
    join(order[2])
    finish_step(order[2])
    join(order[3])
    finish_step(order[3])
    for copy in homing:
        copy.wait_recv()

    def close(index, carry):
        column = pl.ds(pl.multiple_of(index * stride, stride), stride)
        mixture = jnp.dot(
            holds[...],
            returned[:, :, column].reshape(groups * cap, stride),
            preferred_element_type=f32,
        )
        out_ref[:, column] = (updated[:, column] + mixture).astype(bf16)
        return carry

    lax.fori_loop(0, width // stride, close, 0)
    for copy in sent:
        copy.wait_send()


def rope_table(places):
    found = []
    for size in (BROAD_CHANNEL_DIM, THIN_CHANNEL_DIM):
        half = size // 2
        speed = rope_base ** (-np.arange(half, dtype=np.float64) * 2.0 / size)
        angle = places.astype(np.float64)[:, None] * np.tile(speed, 128 // half)[None, :]
        found += [np.cos(angle), np.sin(angle)]
    return np.stack(found).astype(np.float32)


def whole_layer(*arrays):
    staged = arrays[:8]
    (wide_rate, slim_rate, wide_gain, slim_gain, surge, wide_proj, slim_proj) = arrays[8:15]
    (skip, premix, ids, shares, valve, expand, contract) = arrays[15:]
    kind = skip.dtype
    f32 = jnp.float32
    length = surge.shape[0]
    part, width = skip.shape
    count = lax.axis_size("sp")
    groups = GROUPS
    cap = part * groups // count
    valve, expand, contract = valve[0], expand[0], contract[0]
    units = valve.shape[1]
    lanes = 128
    near_table = jnp.asarray(rope_table(np.arange(length)))
    far_table = jnp.asarray(rope_table(np.arange(count) * length).transpose(1, 0, 2))
    any_spec = pl.BlockSpec(memory_space=pl.ANY)
    smem = pl.BlockSpec(memory_space=pltpu.SMEM)
    dma = pltpu.SemaphoreType.DMA
    packed = lanes + lanes // 2

    def kernel(*refs):
        layer_kernel(refs[:8], *refs[8:])

    return pl.pallas_call(
        kernel,
        out_shape=jax.ShapeDtypeStruct(skip.shape, kind),
        in_specs=[any_spec] * 9
        + [VMEM_SPEC] * 2
        + [smem] * 2
        + [VMEM_SPEC] * 2
        + [any_spec] * 3
        + [VMEM_SPEC] * 3
        + [any_spec] * 3,
        out_specs=VMEM_SPEC,
        scratch_shapes=[
            pltpu.VMEM((8, length, 2 * lanes), kind),
            pltpu.VMEM((4, length, lanes), f32),
            pltpu.VMEM((2,) + wide_proj.shape, kind),
            pltpu.VMEM((part, width), kind),
            pltpu.VMEM((4, length, lanes), kind),
            pltpu.VMEM((4, length, lanes), kind),
            pltpu.VMEM((4, length, lanes), kind),
            pltpu.VMEM((length, lanes), f32),
            pltpu.VMEM((length, 4 * lanes), f32),
            pltpu.VMEM((length, 4 * lanes), f32),
            pltpu.VMEM((2, packed, lanes), f32),
            pltpu.VMEM((2, packed, lanes), kind),
            pltpu.VMEM((2, packed, lanes), kind),
            pltpu.VMEM((count, 8, lanes), f32),
            pltpu.VMEM((count, 8, lanes), f32),
            pltpu.VMEM((packed, lanes), kind),
            pltpu.VMEM((groups, packed, lanes), kind),
            pltpu.VMEM((packed, lanes), kind),
            pltpu.VMEM((packed, lanes), kind),
            pltpu.VMEM((3, part, 4 * lanes), kind),
            pltpu.VMEM((4, part, 4 * lanes), kind),
            pltpu.VMEM((part, width), f32),
            pltpu.VMEM((part, width), kind),
            pltpu.VMEM((part, groups * cap), kind),
            pltpu.VMEM((groups, cap, width), kind),
            pltpu.VMEM((groups, cap, width), kind),
            pltpu.VMEM((groups, 4, cap, width), kind),
            pltpu.VMEM((2,) + valve.shape, kind),
            pltpu.VMEM((2,) + expand.shape, kind),
            pltpu.VMEM((2,) + contract.shape, kind),
            pltpu.VMEM((4 * cap, 2 * units), kind),
            pltpu.VMEM((groups, 2, cap, width), f32),
            pltpu.VMEM((groups, 2, cap, width), kind),
            pltpu.VMEM((groups, 2, cap, width), kind),
            pltpu.VMEM((groups, cap, width), kind),
            pltpu.VMEM((groups, cap, width), kind),
            pltpu.VMEM((groups, cap, width), kind),
            dma((16,)),
            dma((3,)),
            dma((3,)),
            dma((count,)),
            dma((count,)),
            dma((2,)),
            dma((2,)),
            dma((groups,)),
            dma((groups,)),
            dma((1,)),
            dma((1,)),
            dma((3,)),
            dma((3,)),
            dma((groups, 2)),
            dma((groups, 2)),
            dma((groups, 6)),
            dma((groups, 6)),
            dma((groups, 4)),
            dma((groups, 4)),
            dma((groups, 2)),
            dma((groups, 2)),
        ],
        compiler_params=pltpu.CompilerParams(
            collective_id=3, has_side_effects=True, vmem_limit_bytes=63 * 1024 * 1024
        ),
        name="whole_layer",
    )(
        *staged,
        near_table,
        far_table,
        surge.reshape(1, -1),
        wide_rate,
        slim_rate,
        wide_gain.reshape(1, -1),
        slim_gain.reshape(1, -1),
        wide_proj,
        slim_proj,
        skip,
        premix.reshape(1, -1),
        ids.T,
        shares.T,
        valve,
        expand,
        contract,
    )


def rotate(payload_tensor, positions):
    channel_dimension = payload_tensor.shape[-1]
    half = channel_dimension // 2
    freq = rope_base ** (-jnp.arange(half, dtype=jnp.float32) * 2.0 / channel_dimension)
    angle = positions.astype(jnp.float32)[:, None, None] * freq[None, None, :]
    cosine = jnp.cos(angle)
    sine = jnp.sin(angle)
    first = payload_tensor[..., :half]
    second = payload_tensor[..., half:]
    return jnp.concatenate([first * cosine - second * sine, first * sine + second * cosine], -1)


def segment_terms(probe_tensor, lookup_tensor, payload_tensor, surge_forgetting, forgetting_speed):
    length = probe_tensor.shape[0]
    segment_tally = jnp.arange(length, dtype=jnp.float32)
    memory_matrix = (
        forgetting_speed[None, :] * segment_tally[:, None] + jnp.cumsum(surge_forgetting)[:, None]
    )
    causal = (segment_tally[:, None] >= segment_tally[None, :])[None]
    level_t = jnp.transpose(memory_matrix)
    gap = level_t[:, :, None] - level_t[:, None, :]
    decay = jnp.where(causal, jnp.exp(jnp.where(causal, gap, 0.0)), 0.0)
    attention_scores = jnp.einsum(
        "szr,yzr->zsy", probe_tensor, lookup_tensor, preferred_element_type=jnp.float32
    )
    weights = (attention_scores * decay).astype(jnp.bfloat16)
    inner = jnp.einsum("htm,mhe->the", weights, payload_tensor, preferred_element_type=jnp.float32)
    factor = jnp.exp(memory_matrix + forgetting_speed[None, :])
    tail = jnp.exp(memory_matrix[-1:, :] - memory_matrix)
    weighted_output = (lookup_tensor.astype(jnp.float32) * tail[:, :, None]).astype(jnp.bfloat16)
    state_update = jnp.einsum(
        "oup,our->upr", weighted_output, payload_tensor, preferred_element_type=jnp.float32
    )
    total = memory_matrix[-1] + forgetting_speed
    return (inner, factor, state_update, total)


def read_state(probe_tensor, state):
    return jnp.einsum(
        "thd,hde->the", probe_tensor.astype(jnp.float32), state, precision=lax.Precision.HIGHEST
    )


def keeping_multiplier(
    probe_source,
    lookup_tensor,
    payload_tensor,
    forgetting_speed,
    surge_forgetting,
    channel_dimension,
    segment_begin,
):
    length = probe_source.shape[0]
    heads = probe_source.shape[1] // channel_dimension
    places = segment_begin + jnp.arange(length, dtype=jnp.int32)
    spun_probe = rotate(
        probe_source.astype(jnp.float32).reshape(length, heads, channel_dimension), places
    ).astype(jnp.bfloat16)
    spun_lookup = (
        rotate(lookup_tensor.astype(jnp.float32).reshape(length, heads, channel_dimension), places)
        * channel_dimension ** (-0.5)
    ).astype(jnp.bfloat16)
    regrouped_payload = payload_tensor.reshape(length, heads, channel_dimension)
    block = min(512, length)
    count = length // block

    def divider_mark(array):
        return array.reshape((count, block) + array.shape[1:])

    state, level, local, reach = None, None, [], []
    for piece in zip(
        divider_mark(spun_probe),
        divider_mark(spun_lookup),
        divider_mark(regrouped_payload),
        divider_mark(surge_forgetting),
    ):
        inner, factor, state_update, total = segment_terms(*piece, forgetting_speed)
        if state is None:
            state, level = state_update, total
        else:
            inner = inner + factor[:, :, None] * read_state(piece[0], state)
            factor = factor * jnp.exp(level)[None, :]
            state, level = jnp.exp(total)[:, None, None] * state + state_update, level + total
        local.append(inner)
        reach.append(factor)
    return (
        spun_probe,
        jnp.concatenate(local, 0),
        jnp.concatenate(reach, 0),
        level,
        state,
    )


def finish(sublayer_final, emission_valve, scaling_coefficients):
    length, heads, channel_dimension = sublayer_final.shape
    normed = sublayer_final * lax.rsqrt(
        jnp.mean(sublayer_final * sublayer_final, -1, keepdims=True) + epsilon
    )
    gated = (
        normed.reshape(length, heads * channel_dimension)
        * scaling_coefficients[None, :]
        * jax.nn.silu(emission_valve.astype(jnp.float32))
    )
    return gated.astype(jnp.bfloat16)


def carried(states, levels):
    place = lax.axis_index("sp")
    count = states.shape[0]
    index = jnp.arange(count, dtype=jnp.int32)
    between = (index[None, :] > index[:, None]) & (index[None, :] < place)
    reach = jnp.sum(jnp.where(between[:, :, None], levels[None, :, :], 0.0), 1)
    weight = jnp.where((index < place)[:, None], jnp.exp(reach), 0.0)
    return jnp.sum(weight[:, :, None, None] * states.astype(jnp.float32), 0)


def slot_positions(chosen, experts, cap):
    listed = chosen.reshape(-1)
    matches = (listed[:, None] == jnp.arange(experts, dtype=jnp.int32)[None, :]).astype(jnp.int32)
    before = jnp.cumsum(matches, 0) - matches
    order = jnp.sum(before * matches, 1)
    return (listed * cap + order).reshape(chosen.shape)


def fill_slots(rows_in, chosen, experts, cap):
    count = rows_in.shape[0]
    places = slot_positions(chosen, experts, cap).reshape(-1)
    owners = jnp.repeat(jnp.arange(count, dtype=jnp.int32), 2)
    source = jnp.full((experts * cap,), count, jnp.int32).at[places].set(owners)
    padded = jnp.concatenate([rows_in, jnp.zeros((1, rows_in.shape[1]), rows_in.dtype)], 0)
    return padded[source].reshape(experts, cap, rows_in.shape[1])


def served(wide, slim, skip, valve):
    return (
        lax.axis_size("sp") * valve.shape[0] == 2 * GROUPS
        and lax.axis_size("tp") == 4
        and wide.shape[1] == slim.shape[1] == 2 * BROAD_CHANNEL_DIM
        and skip.shape[0] == 128
        and wide.shape[0] == 4 * skip.shape[0]
    )


def on_device(
    broad_probe_tensor,
    broad_lookup_tensor,
    broad_payload_tensor,
    broad_emission_valve,
    slim_probe_tensor,
    slim_lookup_tensor,
    slim_payload_tensor,
    slim_emission_valve,
    broad_forgetting_speed,
    slim_forgetting_speed,
    broad_channel_scaling,
    slim_channel_scaling,
    surge_forgetting,
    broad_emission_proj,
    slim_emission_proj,
    skip_stream,
    premix_scaling_coeffs,
    routed_specialist_ids,
    routed_specialist_shares,
    specialist_valve_proj,
    specialist_expand_proj,
    specialist_contract_proj,
):
    length = broad_probe_tensor.shape[0]
    segment_begin = lax.axis_index("sp") * length
    if served(broad_probe_tensor, slim_probe_tensor, skip_stream, specialist_valve_proj):
        return whole_layer(
            broad_probe_tensor,
            broad_lookup_tensor,
            broad_payload_tensor,
            broad_emission_valve,
            slim_probe_tensor,
            slim_lookup_tensor,
            slim_payload_tensor,
            slim_emission_valve,
            broad_forgetting_speed,
            slim_forgetting_speed,
            broad_channel_scaling,
            slim_channel_scaling,
            surge_forgetting,
            broad_emission_proj,
            slim_emission_proj,
            skip_stream,
            premix_scaling_coeffs,
            routed_specialist_ids,
            routed_specialist_shares,
            specialist_valve_proj,
            specialist_expand_proj,
            specialist_contract_proj,
        )
    valve_all = lax.all_gather(specialist_valve_proj[0], "tp")
    expand_all = lax.all_gather(specialist_expand_proj[0], "tp")
    contract_all = lax.all_gather(specialist_contract_proj[0], "tp")
    wide_result = keeping_multiplier(
        broad_probe_tensor,
        broad_lookup_tensor,
        broad_payload_tensor,
        broad_forgetting_speed,
        surge_forgetting,
        BROAD_CHANNEL_DIM,
        segment_begin,
    )
    narrow_result = keeping_multiplier(
        slim_probe_tensor,
        slim_lookup_tensor,
        slim_payload_tensor,
        slim_forgetting_speed,
        surge_forgetting,
        THIN_CHANNEL_DIM,
        segment_begin,
    )
    rows = skip_stream.shape[0]
    width = skip_stream.shape[1]
    experts = lax.axis_size("sp") * specialist_valve_proj.shape[0]
    cap = rows * GROUPS // experts
    pair = experts // GROUPS
    own_ids = lax.dynamic_slice_in_dim(routed_specialist_ids, lax.axis_index("tp") * rows, rows, 0)
    own_weights = lax.dynamic_slice_in_dim(
        routed_specialist_shares, lax.axis_index("tp") * rows, rows, 0
    )
    levels = jnp.concatenate([wide_result[3], narrow_result[3]])
    tile = levels
    tile_size = -(-tile.shape[0] // 1024) * 1024
    tile = jnp.pad(tile, (0, tile_size - tile.shape[0])).reshape(-1, 128)
    packed = jnp.concatenate(
        [wide_result[4].reshape(-1, 128), narrow_result[4].reshape(-1, 128)], 0
    ).astype(jnp.bfloat16)
    states, tiles = exchange(packed, tile)
    count = states.shape[0]
    tiles = tiles.reshape(count, -1)
    wide_heads = wide_result[3].shape[0]
    both_heads = levels.shape[0]
    cut = wide_result[4].size // 128
    incoming_wide = carried(
        states[:, :cut].reshape((count,) + wide_result[4].shape), tiles[:, :wide_heads]
    )
    incoming_narrow = carried(
        states[:, cut:].reshape((count,) + narrow_result[4].shape),
        tiles[:, wide_heads:both_heads],
    )
    mixed_wide = finish(
        wide_result[1] + wide_result[2][:, :, None] * read_state(wide_result[0], incoming_wide),
        broad_emission_valve,
        broad_channel_scaling,
    )
    mixed_narrow = finish(
        narrow_result[1] + narrow_result[2][:, :, None] * read_state(narrow_result[0], incoming_narrow),
        slim_emission_valve,
        slim_channel_scaling,
    )
    rows_wide, rows_narrow = (
        lax.all_to_all(mixed_wide, "tp", split_axis=0, concat_axis=1, tiled=True),
        lax.all_to_all(mixed_narrow, "tp", split_axis=0, concat_axis=1, tiled=True),
    )
    projected = jnp.dot(rows_wide, broad_emission_proj, preferred_element_type=jnp.float32)
    projected = projected + jnp.dot(
        rows_narrow, slim_emission_proj, preferred_element_type=jnp.float32
    )
    updated = skip_stream.astype(jnp.float32) + projected
    scale = lax.rsqrt(jnp.mean(updated * updated, -1, keepdims=True) + epsilon)
    normed = (updated * scale * premix_scaling_coeffs[None, :]).astype(jnp.bfloat16)
    own_places = slot_positions(own_ids, experts, cap)
    slots = lax.all_to_all(
        fill_slots(normed, own_ids, experts, cap), "sp", split_axis=0, concat_axis=0, tiled=True
    ).reshape(-1, width)
    expert_out = None
    for part in range(lax.axis_size("tp")):
        emission_valve = jnp.dot(slots, valve_all[part], preferred_element_type=jnp.float32)
        up = jnp.dot(slots, expand_all[part], preferred_element_type=jnp.float32)
        hidden = (jax.nn.silu(emission_valve) * up).astype(jnp.bfloat16)
        term = jnp.dot(hidden, contract_all[part], preferred_element_type=jnp.float32)
        expert_out = term if expert_out is None else expert_out + term
    returned = lax.all_to_all(
        expert_out.astype(jnp.bfloat16).reshape(experts, cap, width),
        "sp",
        split_axis=0,
        concat_axis=0,
        tiled=True,
    )
    picked = returned.reshape(experts * cap, width)[own_places]
    mixture = jnp.sum(own_weights[:, :, None] * picked.astype(jnp.float32), 1)
    return (updated + mixture).astype(jnp.bfloat16)


def solution(mesh):
    return jax.shard_map(
        on_device,
        mesh=mesh,
        in_specs=(
            P("sp", "tp"),
            P("sp", "tp"),
            P("sp", "tp"),
            P("sp", "tp"),
            P("sp", "tp"),
            P("sp", "tp"),
            P("sp", "tp"),
            P("sp", "tp"),
            P("tp"),
            P("tp"),
            P("tp"),
            P("tp"),
            P("sp"),
            P(),
            P(),
            P(("sp", "tp"), None),
            P(),
            P("sp", None),
            P("sp", None),
            P("sp", None, "tp"),
            P("sp", None, "tp"),
            P("sp", "tp", None),
        ),
        out_specs=P(("sp", "tp"), None),
        check_vma=False,
    )
```

```python
import jax
import jax.numpy as jnp
import numpy as np
from jax import lax
from jax.experimental import pallas as pl
from jax.experimental.pallas import tpu as pltpu
from jax.sharding import PartitionSpec as P

MESH = pl.DeviceIdType.MESH
VMEM_SPEC = pl.BlockSpec(memory_space=pltpu.VMEM)

BROAD_CHANNEL_DIM = 128
THIN_CHANNEL_DIM = 64
GROUPS = 4


rope_base = 10000.0
epsilon = 1e-06


def exchange_kernel(state_ref, tile_ref, states_ref, tiles_ref, send_sem, recv_sem):
    me = lax.axis_index("sp")
    count = states_ref.shape[0]
    barrier = pltpu.get_barrier_semaphore()
    for step in range(1, count):
        pl.semaphore_signal(
            barrier, inc=1, device_id={"sp": lax.rem(me + step, count)}, device_id_type=MESH
        )
    pl.semaphore_wait(barrier, count - 1)
    copies = []
    for step in range(1, count):
        for kind, (src, dst) in enumerate(((state_ref, states_ref), (tile_ref, tiles_ref))):
            copy = pltpu.make_async_remote_copy(
                src_ref=src,
                dst_ref=dst.at[me],
                send_sem=send_sem.at[kind, step],
                recv_sem=recv_sem.at[kind, step],
                device_id={"sp": lax.rem(me + step, count)},
                device_id_type=MESH,
            )
            copy.start()
            copies.append(copy)
    states_ref[me] = state_ref[...]
    tiles_ref[me] = tile_ref[...]
    for copy in copies:
        copy.wait()


def exchange(state, tile):
    count = lax.axis_size("sp")
    return pl.pallas_call(
        exchange_kernel,
        out_shape=(
            jax.ShapeDtypeStruct((count,) + state.shape, state.dtype),
            jax.ShapeDtypeStruct((count,) + tile.shape, tile.dtype),
        ),
        in_specs=[VMEM_SPEC] * 2,
        out_specs=(VMEM_SPEC, VMEM_SPEC),
        scratch_shapes=[
            pltpu.SemaphoreType.DMA((2, count)),
            pltpu.SemaphoreType.DMA((2, count)),
        ],
        compiler_params=pltpu.CompilerParams(collective_id=0, has_side_effects=True),
        name="state_exchange",
    )(state, tile)


def places_of(groups):
    sp = lax.axis_index("sp")
    tp = lax.axis_index("tp")
    core = lax.rem(tp, 2)
    x = lax.rem(sp, 2)
    y = tp // 2
    across_sp = sp + 1 - 2 * x
    across_tp = tp + 2 - 4 * y
    near = {"sp": across_sp + core * (sp - across_sp), "tp": tp + core * (across_tp - tp)}
    side = {"sp": sp + core * (across_sp - sp), "tp": across_tp + core * (tp - across_tp)}
    twin = {"sp": sp, "tp": tp + 1 - 2 * core}
    group = sp // 2
    far = [{"sp": lax.rem(group + step, groups) * 2 + x, "tp": tp} for step in range(groups)]
    return group, x, y, core, near, side, twin, far


def layer_kernel(
    inputs,
    tables_ref,
    turn_ref,
    surge_ref,
    wide_rate,
    slim_rate,
    wide_gain,
    slim_gain,
    wide_proj,
    slim_proj,
    skip_ref,
    premix_ref,
    ids_ref,
    share_ref,
    valve_ref,
    expand_ref,
    contract_ref,
    out_ref,
    staged,
    tables,
    proj,
    skip,
    queries,
    keys,
    faded,
    level,
    inner,
    gates,
    grown,
    grown_out,
    grown_in,
    tile_out,
    tiles,
    plane_out,
    plane_in,
    carry_out,
    carry_in,
    mixed_out,
    mixed,
    updated,
    normed,
    holds,
    rows,
    returned,
    slots,
    valve,
    expand,
    contract,
    hidden,
    kept,
    leave,
    landed,
    joined,
    met,
    back,
    load_sem,
    swap_send,
    swap_recv,
    tile_send,
    tile_recv,
    grown_send,
    grown_recv,
    plane_send,
    plane_recv,
    carry_send,
    carry_recv,
    mixed_send,
    mixed_recv,
    far_send,
    far_recv,
    near_send,
    near_recv,
    fold_send,
    fold_recv,
    home_send,
    home_recv,
):
    f32 = jnp.float32
    bf16 = jnp.bfloat16
    groups, cap, width = rows.shape
    units = valve_ref.shape[1]
    length = staged.shape[1]
    part = skip.shape[0]
    lanes = 128
    blocks = length // part
    count = tiles.shape[0]
    sp = lax.axis_index("sp")
    tp = lax.axis_index("tp")
    group, x, y, core, near, side, twin, far = places_of(groups)
    partner = sp + 1 - 2 * x
    across = tp + 2 - 4 * y
    twin_tp = tp + 1 - 2 * core
    across_twin = twin_tp + 2 - 4 * y

    barrier = pltpu.get_barrier_semaphore()
    friends = [{"sp": lax.rem(sp + step, count), "tp": tp} for step in range(1, count)]
    friends += [{"sp": sp, "tp": other} for other in (across, twin_tp, across_twin)]
    for friend in friends:
        pl.semaphore_signal(barrier, inc=1, device_id=friend, device_id_type=MESH)

    loads = {}

    def load(name, src, dst):
        copy = pltpu.make_async_copy(src, dst, load_sem.at[len(loads)])
        copy.start()
        loads[name] = copy

    for index in (1, 5):
        load(index, inputs[index], staged.at[index])
    load("tables", tables_ref, tables)
    for index in (2, 6, 0, 4, 3, 7):
        load(index, inputs[index], staged.at[index])
    load("skip", skip_ref, skip)

    sent = []

    def send(src, dst, send_sem, recv_sem, device):
        copy = pltpu.make_async_remote_copy(
            src_ref=src,
            dst_ref=dst,
            send_sem=send_sem,
            recv_sem=recv_sem,
            device_id=device,
            device_id_type=MESH,
        )
        copy.start()
        sent.append(copy)
        return copy

    def iota(shape, axis):
        return lax.broadcasted_iota(jnp.int32, shape, axis)

    lane = iota((part, lanes), 1)
    row = iota((part, lanes), 0)
    eye = lane == row
    low_lane = iota((1, lanes), 1) < lanes // 2

    surge = surge_ref[...]
    wide_lane = iota((part, length), 1)
    wide_row = iota((part, length), 0)
    lines = []
    for block in range(blocks):
        column = jnp.sum(
            jnp.where(wide_lane <= wide_row + block * part, surge, 0.0), 1, keepdims=True
        )
        level[pl.ds(block * part, part), :] = jnp.broadcast_to(column, (part, lanes))
        lines.append(jnp.sum(jnp.where(eye, column, 0.0), 0, keepdims=True))
    surge_line = jnp.concatenate(lines, 1)
    surge_total = jnp.broadcast_to(jnp.sum(surge, 1, keepdims=True), (1, lanes))

    rates = [
        jnp.full((1, lanes), wide_rate[0], f32),
        jnp.full((1, lanes), wide_rate[1], f32),
        jnp.where(low_lane, slim_rate[0], slim_rate[1]),
        jnp.where(low_lane, slim_rate[2], slim_rate[3]),
    ]

    def route(block):
        begin = pl.multiple_of(block * part, part)
        ids = ids_ref[0:1, pl.ds(begin, part)]
        weights = share_ref[:, pl.ds(begin, part)]
        first = jnp.sum(jnp.where(eye, ids, 0), 1, keepdims=True)
        weights = [
            jnp.sum(jnp.where(eye, weights[choice : choice + 1], 0.0), 1, keepdims=True)
            for choice in range(2)
        ]
        chosen = lax.shift_right_logical(first, 1)
        named = chosen == lane
        rank = jnp.dot(
            jnp.where(row >= lane, 1.0, 0.0).astype(bf16),
            jnp.where(named, 1.0, 0.0).astype(bf16),
            preferred_element_type=f32,
        )
        order_in = jnp.sum(jnp.where(named, rank, 0.0), 1, keepdims=True).astype(jnp.int32) - 1
        even = first - 2 * chosen == 0
        shares = [
            jnp.where(even, weights[0], weights[1]),
            jnp.where(even, weights[1], weights[0]),
        ]
        return chosen, order_in, shares

    chosen, order_in, _ = route(tp)
    holds[...] = jnp.where(
        chosen * cap + order_in == iota((part, groups * cap), 1), 1.0, 0.0
    ).astype(bf16)
    share_lines = [0.0, 0.0]
    for block_y in range(2):
        chosen, order_in, shares = route(2 * block_y + core)
        here = chosen * (2 * cap) + block_y * cap + order_in == iota((part, 2 * groups * cap), 1)
        for member in range(2):
            share_lines[member] = share_lines[member] + jnp.sum(
                jnp.where(here, shares[member], 0.0), 0, keepdims=True
            )
    top = iota((8, lanes), 0) == 0
    for target in range(count):
        line = share_lines[target % 2][:, (target // 2) * lanes : (target // 2 + 1) * lanes]
        tile_out[target] = jnp.where(top, line, surge_total)
    def turner(size):
        half = size // 2
        low = lax.rem(lane, size) < half
        match = row == jnp.where(low, lane + half, lane - half)
        return jnp.where(match, jnp.where(low, -1.0, 1.0), 0.0).astype(bf16)

    turns = [turner(BROAD_CHANNEL_DIM), turner(THIN_CHANNEL_DIM)]
    scales = [BROAD_CHANNEL_DIM ** (-0.5), THIN_CHANNEL_DIM ** (-0.5)]
    turn = turn_ref[sp]

    def unit_of(index):
        return index // 2, (index % 2) * lanes

    loads["tables"].wait()
    loads[1].wait()
    loads[5].wait()
    last = [rates[unit] * (length - 1) + surge_total for unit in range(4)]

    def turn_keys(block, carry):
        here = pl.ds(pl.multiple_of(block * part, part), part)
        moment = (row + block * part).astype(f32)
        summed = level[here, :]
        for kind in range(2):
            cosine_near = tables[2 * kind, here, :]
            sine_near = tables[2 * kind + 1, here, :]
            cosine_far = turn[2 * kind : 2 * kind + 1]
            sine_far = turn[2 * kind + 1 : 2 * kind + 2]
            cosine = cosine_near * cosine_far - sine_near * sine_far
            sine = sine_near * cosine_far + cosine_near * sine_far
            tables[2 * kind, here, :] = cosine
            tables[2 * kind + 1, here, :] = sine
            for index in range(2):
                unit = 2 * kind + index
                piece = staged[4 * kind + 1, here, index * lanes : (index + 1) * lanes]
                turned = jnp.dot(piece, turns[kind], preferred_element_type=f32)
                key = (
                    (piece.astype(f32) * cosine + turned * sine) * scales[kind]
                ).astype(bf16)
                keys[unit, here, :] = key
                tail = jnp.exp(last[unit] - (rates[unit] * moment + summed))
                faded[unit, here, :] = (key.astype(f32) * tail).astype(bf16)
        return carry

    lax.fori_loop(0, blocks, turn_keys, 0)
    loads[2].wait()
    loads[6].wait()
    for unit in range(4):
        kind, begin = unit_of(unit)
        change = lax.dot_general(
            faded[unit],
            staged[4 * kind + 2, :, begin : begin + lanes],
            (((0,), (0,)), ((), ())),
            preferred_element_type=f32,
        )
        half = unit % 2
        if kind == 0:
            grown[half, :lanes, :] = change
            grown_out[half, :lanes, :] = change.astype(bf16)
        else:
            packed = jnp.where(low_lane, change[: lanes // 2], change[lanes // 2 :])
            grown[half, lanes:, :] = packed
            grown_out[half, lanes:, :] = packed.astype(bf16)
    pl.semaphore_wait(barrier, len(friends))
    tile_copies = []
    for step in range(1, count):
        other = lax.rem(sp + step, count)
        tile_copies.append(
            send(
                tile_out.at[other],
                tiles.at[sp],
                tile_send.at[step],
                tile_recv.at[step],
                {"sp": other, "tp": tp},
            )
        )
    tiles[sp] = tile_out[sp]
    grown_copies = []
    for index in range(2):
        half = 1 - x if index == 0 else x
        grown_copies.append(
            send(
                grown_out.at[half],
                grown_in.at[half],
                grown_send.at[index],
                grown_recv.at[index],
                {"sp": partner, "tp": tp},
            )
        )
    load("wide_proj", wide_proj, proj.at[0])
    load("slim_proj", slim_proj, proj.at[1])
    swaps = []
    for index, (src, dst) in enumerate(
        ((valve_ref, valve), (expand_ref, expand), (contract_ref, contract))
    ):
        load(("expert", index), src, dst.at[core])
        swaps.append(send(src, dst.at[core], swap_send.at[index], swap_recv.at[index], twin))

    loads[0].wait()
    loads[4].wait()

    def turn_queries(block, carry):
        here = pl.ds(pl.multiple_of(block * part, part), part)
        for kind in range(2):
            cosine = tables[2 * kind, here, :]
            sine = tables[2 * kind + 1, here, :]
            for index in range(2):
                piece = staged[4 * kind, here, index * lanes : (index + 1) * lanes]
                turned = jnp.dot(piece, turns[kind], preferred_element_type=f32)
                queries[2 * kind + index, here, :] = (
                    piece.astype(f32) * cosine + turned * sine
                ).astype(bf16)
        return carry

    lax.fori_loop(0, blocks, turn_queries, 0)

    def attend(unit):
        kind, begin = unit_of(unit)
        for block in range(blocks):
            upto = (block + 1) * part
            here = pl.ds(block * part, part)
            query = queries[unit, here, :]
            key = keys[unit, :upto, :]
            value = staged[4 * kind + 2, :upto, begin : begin + lanes]
            spots = iota((part, upto), 1)
            times = iota((part, upto), 0) + block * part
            causal = spots <= times
            apart = (times - spots).astype(f32)
            drop = level[here, 0:1] - surge_line[:, :upto]
            results = []
            for head in range(1 + kind):
                if kind == 0:
                    rate = wide_rate[unit]
                    asked = query
                else:
                    rate = slim_rate[2 * (unit - 2) + head]
                    mine = low_lane if head == 0 else jnp.logical_not(low_lane)
                    asked = jnp.where(mine, query.astype(f32), 0.0).astype(bf16)
                scores = lax.dot_general(
                    asked, key, (((1,), (1,)), ((), ())), preferred_element_type=f32
                )
                gap = apart * rate + drop
                decay = jnp.where(causal, jnp.exp(jnp.where(causal, gap, 0.0)), 0.0)
                results.append(
                    jnp.dot((scores * decay).astype(bf16), value, preferred_element_type=f32)
                )
            result = results[0] if kind == 0 else jnp.where(low_lane, results[0], results[1])
            inner[here, unit * lanes : (unit + 1) * lanes] = result

    attend(0)

    for copy in tile_copies:
        copy.wait_recv()

    def block_level(place, unit):
        return rates[unit] * length + tiles[place, 1:2, :]

    grown_copies[0].wait_recv()
    mine = grown[x]
    other = grown_in[x].astype(f32)
    first = jnp.where(x == 0, mine, other)
    second = jnp.where(x == 0, other, mine)

    def by_half(wide_values, slim_values):
        return (
            jnp.where(x == 0, wide_values[0], wide_values[1]),
            jnp.where(x == 0, slim_values[0], slim_values[1]),
        )

    def weigh(value, pair):
        return jnp.concatenate([value[:lanes] * pair[0], value[lanes:] * pair[1]], 0)

    odd = [jnp.exp(block_level(2 * group + 1, unit)) for unit in range(4)]
    plane_out[...] = (weigh(first, by_half(odd[:2], odd[2:])) + second).astype(bf16)
    plane_copies = []
    for step in range(1, groups):
        plane_copies.append(
            send(
                plane_out,
                plane_in.at[step],
                plane_send.at[step],
                plane_recv.at[step],
                far[step],
            )
        )

    attend(1)
    attend(2)
    attend(3)
    loads[3].wait()
    loads[7].wait()

    def open_gates(block, carry):
        here = pl.ds(pl.multiple_of(block * part, part), part)
        for kind, gain in enumerate((wide_gain, slim_gain)):
            gate = staged[4 * kind + 3, here, :].astype(f32)
            gates[here, 2 * kind * lanes : (2 * kind + 2) * lanes] = gain[...] * jax.nn.silu(gate)
        return carry

    lax.fori_loop(0, blocks, open_gates, 0)
    loads["skip"].wait()
    updated[...] = skip[...].astype(f32)

    carry = jnp.zeros(plane_out.shape, f32)
    reach = [jnp.zeros((1, lanes), f32) for _ in range(4)]
    for step in range(1, groups):
        weight = [jnp.where(group >= step, jnp.exp(reach[unit]), 0.0) for unit in range(4)]
        plane_copies[step - 1].wait_recv()
        carry = carry + weigh(
            plane_in[step].astype(f32), by_half(weight[:2], weight[2:])
        )
        place = lax.rem(group + groups - step, groups)
        for unit in range(4):
            reach[unit] = (
                reach[unit] + block_level(2 * place, unit) + block_level(2 * place + 1, unit)
            )
    carry_out[...] = carry.astype(bf16)
    carry_copy = send(
        carry_out, carry_in, carry_send.at[0], carry_recv.at[0], {"sp": partner, "tp": tp}
    )
    grown_copies[1].wait_recv()
    beside = [
        jnp.where(x == 0, 1.0, jnp.exp(block_level(partner, unit))) for unit in range(4)
    ]
    earlier = jnp.where(x == 0, 0.0, 1.0)
    carry_copy.wait_recv()
    states = [None] * 4
    for half in range(2):
        held = jnp.where(x == half, carry, carry_in[...].astype(f32))
        state = weigh(held, (beside[half], beside[2 + half])) + earlier * grown_in[half].astype(f32)
        states[half] = state[:lanes].astype(bf16)
        slim = state[lanes:]
        states[2 + half] = jnp.concatenate(
            [jnp.where(low_lane, slim, 0.0), jnp.where(low_lane, 0.0, slim)], 0
        ).astype(bf16)

    mixed_copies = []
    for index, owner in enumerate((across, across_twin, twin_tp, tp)):
        begin = pl.multiple_of(owner * part, part)
        here = pl.ds(begin, part)
        moment = (row + begin + 1).astype(f32)
        summed = level[here, :]
        for unit in range(4):
            columns = slice(unit * lanes, (unit + 1) * lanes)
            read = jnp.dot(queries[unit, here, :], states[unit], preferred_element_type=f32)
            factor = jnp.exp(rates[unit] * moment + summed)
            value = inner[here, columns] + factor * read
            square = value * value
            if unit < 2:
                mean = jnp.sum(square, 1, keepdims=True) * (1.0 / BROAD_CHANNEL_DIM)
            else:
                mean = jnp.where(
                    low_lane,
                    jnp.sum(jnp.where(low_lane, square, 0.0), 1, keepdims=True),
                    jnp.sum(jnp.where(low_lane, 0.0, square), 1, keepdims=True),
                ) * (1.0 / THIN_CHANNEL_DIM)
            gated = (value * lax.rsqrt(mean + epsilon) * gates[here, columns]).astype(bf16)
            if index < 3:
                mixed_out[index, :, columns] = gated
            else:
                mixed[tp, :, columns] = gated
        if index < 3:
            mixed_copies.append(
                send(
                    mixed_out.at[index],
                    mixed.at[tp],
                    mixed_send.at[index],
                    mixed_recv.at[index],
                    {"sp": sp, "tp": owner},
                )
            )

    loads["wide_proj"].wait()
    loads["slim_proj"].wait()
    stride = 512
    share_rows = 2 * lanes

    def project(origin):
        above = pl.ds(pl.multiple_of(origin * share_rows, share_rows), share_rows)
        wide = mixed[origin, :, :share_rows]
        slim = mixed[origin, :, share_rows:]

        def one(index, carry):
            column = pl.ds(pl.multiple_of(index * stride, stride), stride)
            updated[:, column] += jnp.dot(
                wide, proj[0, above, column], preferred_element_type=f32
            ) + jnp.dot(slim, proj[1, above, column], preferred_element_type=f32)
            return carry

        lax.fori_loop(0, width // stride, one, 0)

    project(tp)
    mixed_copies[2].wait_recv()
    project(twin_tp)
    mixed_copies[0].wait_recv()
    project(across)
    mixed_copies[1].wait_recv()
    project(across_twin)
    square = jnp.zeros((part, lanes), f32)
    for begin in range(0, width, lanes):
        piece = updated[:, begin : begin + lanes]
        square = square + piece * piece
    scale = lax.rsqrt(jnp.sum(square, 1, keepdims=True) * (1.0 / width) + epsilon)

    def place_rows(index, carry):
        column = pl.ds(pl.multiple_of(index * stride, stride), stride)
        piece = (updated[:, column] * scale * premix_ref[:, column]).astype(bf16)
        spread_rows = lax.dot_general(
            holds[...], piece, (((0,), (0,)), ((), ())), preferred_element_type=f32
        )
        rows[:, :, column] = spread_rows.reshape(groups, cap, stride).astype(bf16)
        return carry

    lax.fori_loop(0, width // stride, place_rows, 0)

    order = [1, 2, 3, 0]
    pairs = [lax.rem(group + groups - step, groups) for step in range(groups)]
    seen_as = list(range(groups))
    away = [{"sp": 2 * pairs[step] + x, "tp": tp} for step in range(groups)]
    piece_rows = cap // 2

    def piece(portion):
        return pl.ds(portion * piece_rows, piece_rows)

    for step in order[:3]:
        for portion in range(2):
            send(
                rows.at[lax.rem(group + step, groups), piece(portion)],
                slots.at[step, 0, piece(portion)],
                far_send.at[step, portion],
                far_recv.at[step, portion],
                far[step],
            )

    def arrived(dst, recv_sem, step):
        pltpu.make_async_remote_copy(
            src_ref=dst,
            dst_ref=dst,
            send_sem=far_send.at[0, 0],
            recv_sem=recv_sem,
            device_id=away[step],
            device_id_type=MESH,
        ).wait_recv()

    own = {}

    def spread(step, portion):
        here = piece(portion)
        if step > 0:
            arrived(slots.at[step, 0, here], far_recv.at[step, portion], step)
        src = rows.at[group, here] if step == 0 else slots.at[step, 0, here]
        for place, device in ((1, near), (2, side)):
            own[step, place, portion] = send(
                src,
                slots.at[step, place, here],
                near_send.at[step, 2 * place - 2 + portion],
                near_recv.at[step, 2 * place - 2 + portion],
                device,
            )

    def forward(step, portion):
        here = piece(portion)
        own[step, 1, portion].wait_recv()
        own[step, 3, portion] = send(
            slots.at[step, 1, here],
            slots.at[step, 3, here],
            near_send.at[step, 4 + portion],
            near_recv.at[step, 4 + portion],
            side,
        )

    spread(0, 0)
    spread(0, 1)
    slots[0, 0] = rows[group]
    forward(0, 0)
    forward(0, 1)
    spread(1, 0)
    spread(1, 1)
    forward(1, 0)
    forward(1, 1)
    near_x = 1 - x + core * (2 * x - 1)
    near_y = y + core * (1 - 2 * y)

    def shares_for(step):
        origin = pairs[step]
        found = []
        for at_x, at_y in ((x, y), (near_x, near_y), (1 - near_x, 1 - near_y), (1 - x, 1 - y)):
            line = tiles[2 * origin + at_x, 0:1, :]
            pick = iota((cap, lanes), 1) == iota((cap, lanes), 0) + at_y * cap
            found.append(jnp.sum(jnp.where(pick, line, 0.0), 1, keepdims=True))
        return jnp.concatenate(found, 0)

    tile = 256

    def widen(step, portion):
        share = shares_for(step)
        batch = slots[step].reshape(4 * cap, width)

        def one(index, carry):
            half = index // (units // tile)
            begin = pl.multiple_of(lax.rem(index, units // tile) * tile, tile)
            gate = jnp.dot(batch, valve[half, :, pl.ds(begin, tile)], preferred_element_type=f32)
            up = jnp.dot(batch, expand[half, :, pl.ds(begin, tile)], preferred_element_type=f32)
            place = pl.multiple_of(index * tile, tile)
            hidden[int(step == 0), :, pl.ds(place, tile)] = (
                jax.nn.silu(gate) * up * share
            ).astype(bf16)
            return carry

        count_tiles = 2 * units // tile // 2
        lax.fori_loop(portion * count_tiles, (portion + 1) * count_tiles, one, 0)

    folding = {}
    joining = {}
    chunks = {0: 2, 1: 2, 2: 2, 3: 2}

    def columns_of(step, portion):
        span = width // chunks[step]
        return pl.ds(portion * span, span)

    def narrow(step, portions):
        for portion in portions:

            def one(index, carry):
                column = pl.ds(pl.multiple_of(index * stride, stride), stride)
                made = jnp.dot(
                    hidden[int(step == 0), :, :units], contract[0, :, column], preferred_element_type=f32
                ) + jnp.dot(
                    hidden[int(step == 0), :, units:], contract[1, :, column], preferred_element_type=f32)
                kept[step, :, :, column] = made[: 2 * cap].reshape(2, cap, stride)
                leave[step, :, :, column] = made[2 * cap :].reshape(2, cap, stride).astype(bf16)
                return carry

            tiles_in = width // chunks[step] // stride
            lax.fori_loop(portion * tiles_in, (portion + 1) * tiles_in, one, 0)
            column = columns_of(step, portion)
            folding[step, portion] = send(
                leave.at[step, :, :, column],
                landed.at[step, :, :, column],
                fold_send.at[step, portion],
                fold_recv.at[step, portion],
                side,
            )

    def join(step):
        for portion in range(chunks[step]):
            column = columns_of(step, portion)
            folding[step, portion].wait_recv()
            joined[step, :, column] = (
                kept[step, 1, :, column] + landed[step, 1, :, column].astype(f32)
            ).astype(bf16)
            joining[step, portion] = send(
                joined.at[step, :, column],
                met.at[step, :, column],
                fold_send.at[step, 4 + portion],
                fold_recv.at[step, 4 + portion],
                near,
            )

    def finish_part(step, portion):
        column = columns_of(step, portion)
        joining[step, portion].wait_recv()
        total = (
            kept[step, 0, :, column]
            + landed[step, 0, :, column].astype(f32)
            + met[step, :, column].astype(f32)
        ).astype(bf16)
        if step == 0:
            returned[group, :, column] = total
        else:
            back[step, :, column] = total
            send(
                back.at[step, :, column],
                returned.at[group, :, column],
                home_send.at[step, portion],
                home_recv.at[seen_as[step], portion],
                away[step],
            )

    def finish_step(step):
        for portion in range(chunks[step]):
            finish_part(step, portion)

    def gathered(step):
        for portion in range(2):
            own[step, 2, portion].wait_recv()
            own[step, 3, portion].wait_recv()

    for index in range(3):
        loads[("expert", index)].wait()
        swaps[index].wait_recv()
    gathered(0)
    widen(0, 0)
    spread(3, 0)
    spread(3, 1)
    widen(0, 1)
    spread(2, 0)
    spread(2, 1)
    gathered(1)
    widen(1, 0)
    forward(3, 0)
    forward(3, 1)
    widen(1, 1)
    narrow(1, [0, 1])
    gathered(3)
    widen(3, 0)
    forward(2, 0)
    forward(2, 1)
    widen(3, 1)
    narrow(3, [0, 1])
    join(1)
    gathered(2)
    widen(2, 0)
    finish_step(1)
    widen(2, 1)
    narrow(2, [0, 1])
    join(3)
    narrow(0, [0, 1])
    finish_step(3)
    join(2)
    finish_step(2)
    join(0)
    for step in range(1, groups):
        for portion in range(chunks[step]):
            arrived(
                returned.at[lax.rem(group + step, groups), :, columns_of(step, portion)],
                home_recv.at[step, portion],
                step,
            )
    for portion in range(2):
        finish_part(0, portion)
        column = pl.ds(portion * (width // 2), width // 2)
        mixture = jnp.dot(
            holds[...],
            returned[:, :, column].reshape(groups * cap, -1),
            preferred_element_type=f32,
        )
        out_ref[:, column] = (updated[:, column] + mixture).astype(bf16)
    for copy in sent:
        copy.wait_send()


def rope_table(places):
    found = []
    for size in (BROAD_CHANNEL_DIM, THIN_CHANNEL_DIM):
        half = size // 2
        speed = rope_base ** (-np.arange(half, dtype=np.float64) * 2.0 / size)
        angle = places.astype(np.float64)[:, None] * np.tile(speed, 128 // half)[None, :]
        found += [np.cos(angle), np.sin(angle)]
    return np.stack(found).astype(np.float32)


def whole_layer(*arrays):
    staged = arrays[:8]
    (wide_rate, slim_rate, wide_gain, slim_gain, surge, wide_proj, slim_proj) = arrays[8:15]
    (skip, premix, ids, shares, valve, expand, contract) = arrays[15:]
    kind = skip.dtype
    f32 = jnp.float32
    length = surge.shape[0]
    part, width = skip.shape
    count = lax.axis_size("sp")
    groups = GROUPS
    cap = part * groups // count
    valve, expand, contract = valve[0], expand[0], contract[0]
    units = valve.shape[1]
    lanes = 128
    near_table = jnp.asarray(rope_table(np.arange(length)))
    far_table = jnp.asarray(rope_table(np.arange(count) * length).transpose(1, 0, 2))
    any_spec = pl.BlockSpec(memory_space=pl.ANY)
    smem = pl.BlockSpec(memory_space=pltpu.SMEM)
    dma = pltpu.SemaphoreType.DMA
    packed = lanes + lanes // 2

    def kernel(*refs):
        layer_kernel(refs[:8], *refs[8:])

    return pl.pallas_call(
        kernel,
        out_shape=jax.ShapeDtypeStruct(skip.shape, kind),
        in_specs=[any_spec] * 9
        + [VMEM_SPEC] * 2
        + [smem] * 2
        + [VMEM_SPEC] * 2
        + [any_spec] * 3
        + [VMEM_SPEC] * 3
        + [any_spec] * 3,
        out_specs=VMEM_SPEC,
        scratch_shapes=[
            pltpu.VMEM((8, length, 2 * lanes), kind),
            pltpu.VMEM((4, length, lanes), f32),
            pltpu.VMEM((2,) + wide_proj.shape, kind),
            pltpu.VMEM((part, width), kind),
            pltpu.VMEM((4, length, lanes), kind),
            pltpu.VMEM((4, length, lanes), kind),
            pltpu.VMEM((4, length, lanes), kind),
            pltpu.VMEM((length, lanes), f32),
            pltpu.VMEM((length, 4 * lanes), f32),
            pltpu.VMEM((length, 4 * lanes), f32),
            pltpu.VMEM((2, packed, lanes), f32),
            pltpu.VMEM((2, packed, lanes), kind),
            pltpu.VMEM((2, packed, lanes), kind),
            pltpu.VMEM((count, 8, lanes), f32),
            pltpu.VMEM((count, 8, lanes), f32),
            pltpu.VMEM((packed, lanes), kind),
            pltpu.VMEM((groups, packed, lanes), kind),
            pltpu.VMEM((packed, lanes), kind),
            pltpu.VMEM((packed, lanes), kind),
            pltpu.VMEM((3, part, 4 * lanes), kind),
            pltpu.VMEM((4, part, 4 * lanes), kind),
            pltpu.VMEM((part, width), f32),
            pltpu.VMEM((part, width), kind),
            pltpu.VMEM((part, groups * cap), kind),
            pltpu.VMEM((groups, cap, width), kind),
            pltpu.VMEM((groups, cap, width), kind),
            pltpu.VMEM((groups, 4, cap, width), kind),
            pltpu.VMEM((2,) + valve.shape, kind),
            pltpu.VMEM((2,) + expand.shape, kind),
            pltpu.VMEM((2,) + contract.shape, kind),
            pltpu.VMEM((2, 4 * cap, 2 * units), kind),
            pltpu.VMEM((groups, 2, cap, width), f32),
            pltpu.VMEM((groups, 2, cap, width), kind),
            pltpu.VMEM((groups, 2, cap, width), kind),
            pltpu.VMEM((groups, cap, width), kind),
            pltpu.VMEM((groups, cap, width), kind),
            pltpu.VMEM((groups, cap, width), kind),
            dma((16,)),
            dma((3,)),
            dma((3,)),
            dma((count,)),
            dma((count,)),
            dma((2,)),
            dma((2,)),
            dma((groups,)),
            dma((groups,)),
            dma((1,)),
            dma((1,)),
            dma((3,)),
            dma((3,)),
            dma((groups, 2)),
            dma((groups, 2)),
            dma((groups, 6)),
            dma((groups, 6)),
            dma((groups, 8)),
            dma((groups, 8)),
            dma((groups, 4)),
            dma((groups, 4)),
        ],
        compiler_params=pltpu.CompilerParams(
            collective_id=3, has_side_effects=True, vmem_limit_bytes=63 * 1024 * 1024
        ),
        name="whole_layer",
    )(
        *staged,
        near_table,
        far_table,
        surge.reshape(1, -1),
        wide_rate,
        slim_rate,
        wide_gain.reshape(1, -1),
        slim_gain.reshape(1, -1),
        wide_proj,
        slim_proj,
        skip,
        premix.reshape(1, -1),
        ids.T,
        shares.T,
        valve,
        expand,
        contract,
    )


def rotate(payload_tensor, positions):
    channel_dimension = payload_tensor.shape[-1]
    half = channel_dimension // 2
    freq = rope_base ** (-jnp.arange(half, dtype=jnp.float32) * 2.0 / channel_dimension)
    angle = positions.astype(jnp.float32)[:, None, None] * freq[None, None, :]
    cosine = jnp.cos(angle)
    sine = jnp.sin(angle)
    first = payload_tensor[..., :half]
    second = payload_tensor[..., half:]
    return jnp.concatenate([first * cosine - second * sine, first * sine + second * cosine], -1)


def segment_terms(probe_tensor, lookup_tensor, payload_tensor, surge_forgetting, forgetting_speed):
    length = probe_tensor.shape[0]
    segment_tally = jnp.arange(length, dtype=jnp.float32)
    memory_matrix = (
        forgetting_speed[None, :] * segment_tally[:, None] + jnp.cumsum(surge_forgetting)[:, None]
    )
    causal = (segment_tally[:, None] >= segment_tally[None, :])[None]
    level_t = jnp.transpose(memory_matrix)
    gap = level_t[:, :, None] - level_t[:, None, :]
    decay = jnp.where(causal, jnp.exp(jnp.where(causal, gap, 0.0)), 0.0)
    attention_scores = jnp.einsum(
        "szr,yzr->zsy", probe_tensor, lookup_tensor, preferred_element_type=jnp.float32
    )
    weights = (attention_scores * decay).astype(jnp.bfloat16)
    inner = jnp.einsum("htm,mhe->the", weights, payload_tensor, preferred_element_type=jnp.float32)
    factor = jnp.exp(memory_matrix + forgetting_speed[None, :])
    tail = jnp.exp(memory_matrix[-1:, :] - memory_matrix)
    weighted_output = (lookup_tensor.astype(jnp.float32) * tail[:, :, None]).astype(jnp.bfloat16)
    state_update = jnp.einsum(
        "oup,our->upr", weighted_output, payload_tensor, preferred_element_type=jnp.float32
    )
    total = memory_matrix[-1] + forgetting_speed
    return (inner, factor, state_update, total)


def read_state(probe_tensor, state):
    return jnp.einsum(
        "thd,hde->the", probe_tensor.astype(jnp.float32), state, precision=lax.Precision.HIGHEST
    )


def keeping_multiplier(
    probe_source,
    lookup_tensor,
    payload_tensor,
    forgetting_speed,
    surge_forgetting,
    channel_dimension,
    segment_begin,
):
    length = probe_source.shape[0]
    heads = probe_source.shape[1] // channel_dimension
    places = segment_begin + jnp.arange(length, dtype=jnp.int32)
    spun_probe = rotate(
        probe_source.astype(jnp.float32).reshape(length, heads, channel_dimension), places
    ).astype(jnp.bfloat16)
    spun_lookup = (
        rotate(lookup_tensor.astype(jnp.float32).reshape(length, heads, channel_dimension), places)
        * channel_dimension ** (-0.5)
    ).astype(jnp.bfloat16)
    regrouped_payload = payload_tensor.reshape(length, heads, channel_dimension)
    block = min(512, length)
    count = length // block

    def divider_mark(array):
        return array.reshape((count, block) + array.shape[1:])

    state, level, local, reach = None, None, [], []
    for piece in zip(
        divider_mark(spun_probe),
        divider_mark(spun_lookup),
        divider_mark(regrouped_payload),
        divider_mark(surge_forgetting),
    ):
        inner, factor, state_update, total = segment_terms(*piece, forgetting_speed)
        if state is None:
            state, level = state_update, total
        else:
            inner = inner + factor[:, :, None] * read_state(piece[0], state)
            factor = factor * jnp.exp(level)[None, :]
            state, level = jnp.exp(total)[:, None, None] * state + state_update, level + total
        local.append(inner)
        reach.append(factor)
    return (
        spun_probe,
        jnp.concatenate(local, 0),
        jnp.concatenate(reach, 0),
        level,
        state,
    )


def finish(sublayer_final, emission_valve, scaling_coefficients):
    length, heads, channel_dimension = sublayer_final.shape
    normed = sublayer_final * lax.rsqrt(
        jnp.mean(sublayer_final * sublayer_final, -1, keepdims=True) + epsilon
    )
    gated = (
        normed.reshape(length, heads * channel_dimension)
        * scaling_coefficients[None, :]
        * jax.nn.silu(emission_valve.astype(jnp.float32))
    )
    return gated.astype(jnp.bfloat16)


def carried(states, levels):
    place = lax.axis_index("sp")
    count = states.shape[0]
    index = jnp.arange(count, dtype=jnp.int32)
    between = (index[None, :] > index[:, None]) & (index[None, :] < place)
    reach = jnp.sum(jnp.where(between[:, :, None], levels[None, :, :], 0.0), 1)
    weight = jnp.where((index < place)[:, None], jnp.exp(reach), 0.0)
    return jnp.sum(weight[:, :, None, None] * states.astype(jnp.float32), 0)


def slot_positions(chosen, experts, cap):
    listed = chosen.reshape(-1)
    matches = (listed[:, None] == jnp.arange(experts, dtype=jnp.int32)[None, :]).astype(jnp.int32)
    before = jnp.cumsum(matches, 0) - matches
    order = jnp.sum(before * matches, 1)
    return (listed * cap + order).reshape(chosen.shape)


def fill_slots(rows_in, chosen, experts, cap):
    count = rows_in.shape[0]
    places = slot_positions(chosen, experts, cap).reshape(-1)
    owners = jnp.repeat(jnp.arange(count, dtype=jnp.int32), 2)
    source = jnp.full((experts * cap,), count, jnp.int32).at[places].set(owners)
    padded = jnp.concatenate([rows_in, jnp.zeros((1, rows_in.shape[1]), rows_in.dtype)], 0)
    return padded[source].reshape(experts, cap, rows_in.shape[1])


def served(wide, slim, skip, valve):
    return (
        lax.axis_size("sp") * valve.shape[0] == 2 * GROUPS
        and lax.axis_size("tp") == 4
        and wide.shape[1] == slim.shape[1] == 2 * BROAD_CHANNEL_DIM
        and skip.shape[0] == 128
        and wide.shape[0] == 4 * skip.shape[0]
    )


def on_device(
    broad_probe_tensor,
    broad_lookup_tensor,
    broad_payload_tensor,
    broad_emission_valve,
    slim_probe_tensor,
    slim_lookup_tensor,
    slim_payload_tensor,
    slim_emission_valve,
    broad_forgetting_speed,
    slim_forgetting_speed,
    broad_channel_scaling,
    slim_channel_scaling,
    surge_forgetting,
    broad_emission_proj,
    slim_emission_proj,
    skip_stream,
    premix_scaling_coeffs,
    routed_specialist_ids,
    routed_specialist_shares,
    specialist_valve_proj,
    specialist_expand_proj,
    specialist_contract_proj,
):
    length = broad_probe_tensor.shape[0]
    segment_begin = lax.axis_index("sp") * length
    if served(broad_probe_tensor, slim_probe_tensor, skip_stream, specialist_valve_proj):
        return whole_layer(
            broad_probe_tensor,
            broad_lookup_tensor,
            broad_payload_tensor,
            broad_emission_valve,
            slim_probe_tensor,
            slim_lookup_tensor,
            slim_payload_tensor,
            slim_emission_valve,
            broad_forgetting_speed,
            slim_forgetting_speed,
            broad_channel_scaling,
            slim_channel_scaling,
            surge_forgetting,
            broad_emission_proj,
            slim_emission_proj,
            skip_stream,
            premix_scaling_coeffs,
            routed_specialist_ids,
            routed_specialist_shares,
            specialist_valve_proj,
            specialist_expand_proj,
            specialist_contract_proj,
        )
    valve_all = lax.all_gather(specialist_valve_proj[0], "tp")
    expand_all = lax.all_gather(specialist_expand_proj[0], "tp")
    contract_all = lax.all_gather(specialist_contract_proj[0], "tp")
    wide_result = keeping_multiplier(
        broad_probe_tensor,
        broad_lookup_tensor,
        broad_payload_tensor,
        broad_forgetting_speed,
        surge_forgetting,
        BROAD_CHANNEL_DIM,
        segment_begin,
    )
    narrow_result = keeping_multiplier(
        slim_probe_tensor,
        slim_lookup_tensor,
        slim_payload_tensor,
        slim_forgetting_speed,
        surge_forgetting,
        THIN_CHANNEL_DIM,
        segment_begin,
    )
    rows = skip_stream.shape[0]
    width = skip_stream.shape[1]
    experts = lax.axis_size("sp") * specialist_valve_proj.shape[0]
    cap = rows * GROUPS // experts
    pair = experts // GROUPS
    own_ids = lax.dynamic_slice_in_dim(routed_specialist_ids, lax.axis_index("tp") * rows, rows, 0)
    own_weights = lax.dynamic_slice_in_dim(
        routed_specialist_shares, lax.axis_index("tp") * rows, rows, 0
    )
    levels = jnp.concatenate([wide_result[3], narrow_result[3]])
    tile = levels
    tile_size = -(-tile.shape[0] // 1024) * 1024
    tile = jnp.pad(tile, (0, tile_size - tile.shape[0])).reshape(-1, 128)
    packed = jnp.concatenate(
        [wide_result[4].reshape(-1, 128), narrow_result[4].reshape(-1, 128)], 0
    ).astype(jnp.bfloat16)
    states, tiles = exchange(packed, tile)
    count = states.shape[0]
    tiles = tiles.reshape(count, -1)
    wide_heads = wide_result[3].shape[0]
    both_heads = levels.shape[0]
    cut = wide_result[4].size // 128
    incoming_wide = carried(
        states[:, :cut].reshape((count,) + wide_result[4].shape), tiles[:, :wide_heads]
    )
    incoming_narrow = carried(
        states[:, cut:].reshape((count,) + narrow_result[4].shape),
        tiles[:, wide_heads:both_heads],
    )
    mixed_wide = finish(
        wide_result[1] + wide_result[2][:, :, None] * read_state(wide_result[0], incoming_wide),
        broad_emission_valve,
        broad_channel_scaling,
    )
    mixed_narrow = finish(
        narrow_result[1] + narrow_result[2][:, :, None] * read_state(narrow_result[0], incoming_narrow),
        slim_emission_valve,
        slim_channel_scaling,
    )
    rows_wide, rows_narrow = (
        lax.all_to_all(mixed_wide, "tp", split_axis=0, concat_axis=1, tiled=True),
        lax.all_to_all(mixed_narrow, "tp", split_axis=0, concat_axis=1, tiled=True),
    )
    projected = jnp.dot(rows_wide, broad_emission_proj, preferred_element_type=jnp.float32)
    projected = projected + jnp.dot(
        rows_narrow, slim_emission_proj, preferred_element_type=jnp.float32
    )
    updated = skip_stream.astype(jnp.float32) + projected
    scale = lax.rsqrt(jnp.mean(updated * updated, -1, keepdims=True) + epsilon)
    normed = (updated * scale * premix_scaling_coeffs[None, :]).astype(jnp.bfloat16)
    own_places = slot_positions(own_ids, experts, cap)
    slots = lax.all_to_all(
        fill_slots(normed, own_ids, experts, cap), "sp", split_axis=0, concat_axis=0, tiled=True
    ).reshape(-1, width)
    expert_out = None
    for part in range(lax.axis_size("tp")):
        emission_valve = jnp.dot(slots, valve_all[part], preferred_element_type=jnp.float32)
        up = jnp.dot(slots, expand_all[part], preferred_element_type=jnp.float32)
        hidden = (jax.nn.silu(emission_valve) * up).astype(jnp.bfloat16)
        term = jnp.dot(hidden, contract_all[part], preferred_element_type=jnp.float32)
        expert_out = term if expert_out is None else expert_out + term
    returned = lax.all_to_all(
        expert_out.astype(jnp.bfloat16).reshape(experts, cap, width),
        "sp",
        split_axis=0,
        concat_axis=0,
        tiled=True,
    )
    picked = returned.reshape(experts * cap, width)[own_places]
    mixture = jnp.sum(own_weights[:, :, None] * picked.astype(jnp.float32), 1)
    return (updated + mixture).astype(jnp.bfloat16)


def solution(mesh):
    return jax.shard_map(
        on_device,
        mesh=mesh,
        in_specs=(
            P("sp", "tp"),
            P("sp", "tp"),
            P("sp", "tp"),
            P("sp", "tp"),
            P("sp", "tp"),
            P("sp", "tp"),
            P("sp", "tp"),
            P("sp", "tp"),
            P("tp"),
            P("tp"),
            P("tp"),
            P("tp"),
            P("sp"),
            P(),
            P(),
            P(("sp", "tp"), None),
            P(),
            P("sp", None),
            P("sp", None),
            P("sp", None, "tp"),
            P("sp", None, "tp"),
            P("sp", "tp", None),
        ),
        out_specs=P(("sp", "tp"), None),
        check_vma=False,
    )
```
